512 devices in a mesh: sp: 32 (over z, x), tp: 16 (over y, core).
Axes of the slice: x: 4, y: 8, z: 8, core: 2. Of those that a mesh axis runs over, the one named last changes fastest.
Arguments:
- queries: bfloat16 [4096, 2048], P('sp', 'tp'), may hold values from -440 to 440
- key_rows: bfloat16 [4096, 1024], P('sp', 'tp'), may hold values from -6 to 6
- value_rows: bfloat16 [4096, 1024], P('sp', 'tp'), may hold values from -6 to 6
- sink_logits: float32 [32], P('tp'), may hold values from -6 to 6
- out_weight: bfloat16 [2048, 2048], P('tp'), may hold values from -0.125 to 0.125
- residual: bfloat16 [4096, 2048], P('sp'), may hold values from -3 to 3
- norm_gain: float32 [2048], replicated, may hold values from 0.1 to 1.9
- routes: int32 [4096, 2], P('sp'), may hold values from 0 to 31, all different within a row; in each aligned block of 128 rows (0 to 127, 128 to 255, ...) at most 16 rows name the same one
- route_weights: float32 [4096, 2], P('sp'), may hold values from 0.2 to 1
- gate_weight: bfloat16 [32, 2048, 4096], P('sp', None, 'tp'), may hold values from -0.125 to 0.125
- up_weight: bfloat16 [32, 2048, 4096], P('sp', None, 'tp'), may hold values from -0.125 to 0.125
- down_weight: bfloat16 [32, 4096, 2048], P('sp', 'tp'), may hold values from -0.09375 to 0.09375
Outputs:
- layer_out: bfloat16 [4096, 2048], P('sp')
The draws below stay inside these ranges and needn't reach their ends.
Inputs may be any that keep to these rules, and one draw needn't show every extreme that they name: `routes`: each row names 2 different experts. In each aligned block of 128 rows (the rows of one index of sp) no expert is named by more than 16 rows, a bound that some block reaches.
All inputs are finite; a program needn't handle non-finite values.
Results may differ from the reference program's by a relative error of at most 0.02.
Values may be sent and summed in bfloat16 or wider, within the bound.
A program may use at most 64 MiB of HBM per device.

```python
import math
import jax
import jax.numpy as jnp
import numpy as np
from jax import lax

D = 2048
HEAD_DIM = 64
QH = 32
KVH = 16
WINDOW = 128
FF = 4096
TOP = 2
TOK_DEV = 128
TOKENS = 4096
EXPERTS = 32
CAP = 16
N_SP = 32
N_TP = 16


def plant_keys(key):
    key_draw = jax.random.normal(jax.random.fold_in(key, 7), (TOKENS, KVH * HEAD_DIM), jnp.float32)
    return jnp.clip(key_draw, -6.0, 6.0)


def draw_key_rows(key, part):
    key_draw = plant_keys(key)
    return key_draw.astype(jnp.bfloat16)


def draw_queries(key, part):
    base = jax.random.normal(jax.random.fold_in(key, 8), (TOKENS, QH * HEAD_DIM), jnp.float32)
    base = jnp.clip(base, -6.0, 6.0)
    return base.astype(jnp.bfloat16)


def levels(key, extent, cuts, smallest, top_value):
    level = 1.0
    for axis_at, shards_of in cuts:
        steps = jax.random.uniform(jax.random.fold_in(jax.random.fold_in(key, 6), axis_at), (shards_of,), jnp.float32, smallest / len(cuts), top_value / len(cuts))
        level = level * jnp.repeat(jnp.exp(steps), extent[axis_at] // shards_of).reshape((-1,) + (1,) * (len(extent) - 1 - axis_at))
    return level


def deal_out(rng, own, number, rows, amount, top, limit, skew):
    ranking = jax.random.permutation(rng, amount)
    heavy_load, common = portions_of(amount, rows * top, limit, skew, True), portions_of(amount, rows * top, limit, skew, False)
    places = jnp.arange(amount)

    def named(tallies, turn):
        used = int((tallies > 0).sum())
        fixed = max(1, used // 4)
        moved = fixed + (places - fixed + turn * (used - fixed)) % max(1, amount - fixed)
        return jnp.zeros((amount,), jnp.int32).at[ranking[jnp.where(places < fixed, places, moved)]].set(jnp.asarray(tallies, jnp.int32))

    tallies = jnp.where(number % 4 == 0, named(heavy_load, number // 4), named(common, number - number // 4 - 1))
    mixed = jax.random.permutation(jax.random.fold_in(own, 3), amount)
    source_of, taker = mixed[0:amount // 2 * 2:2], mixed[1:amount // 2 * 2:2]
    margin = jnp.minimum(tallies[source_of] - 1, limit - tallies[taker]) // 2
    margin = jnp.where((source_of == ranking[0]) | (taker == ranking[0]) | (tallies[taker] == 0), 0, jnp.maximum(margin, 0))
    moved = jax.random.randint(jax.random.fold_in(own, 4), (amount // 2,), 0, 1 << 20) % (margin + 1)
    tallies = tallies.at[source_of].add(-moved).at[taker].add(moved)
    items = jnp.searchsorted(jnp.cumsum(tallies), jnp.arange(rows * top), side="right").astype(jnp.int32)
    grid = items.reshape(top, rows).T
    grid = grid[jax.random.permutation(jax.random.fold_in(own, 1), rows)]
    turn = jax.random.randint(jax.random.fold_in(own, 2), (rows, 1), 0, top)
    return jnp.take_along_axis(grid, (jnp.arange(top)[None, :] + turn) % top, axis=1)


def portions_of(amount, total, limit, slope, full):
    weights = [(1 << 20) // math.isqrt(standing ** slope) + 1 for standing in range(1, amount + 1)]
    largest = limit if full else min(limit, max(-(-total // amount), total * weights[0] // sum(weights)))
    least = 1 if total - largest >= amount - 1 else 0
    counts, surplus = [largest] + [least] * (amount - 1), total - largest - least * (amount - 1)
    while surplus > 0:
        movable = [i for i in range(1, amount) if counts[i] < largest] or [i for i in range(1, amount) if counts[i] < limit]
        whole, left = sum([weights[i] for i in movable]), surplus
        for i in movable:
            addition = min(limit - counts[i], max(1, left * weights[i] // whole), surplus)
            counts[i] = counts[i] + addition
            surplus = surplus - addition
    return np.array(counts)


def noise(rng, extent, deviation, limit, shards=(), kind=jnp.bfloat16):
    level = levels(rng, extent, shards, -0.22, 0.18) if shards else 1.0
    result = jax.random.normal(rng, extent, jnp.float32) * deviation * level
    return jnp.minimum(jnp.maximum(result, -limit), limit).astype(kind)


def setup_inputs(seed: int = 0) -> dict:
    key_of = jax.random.split(jax.random.key(seed), 13)
    queries = draw_queries(jax.random.fold_in(key_of[12], 71), 0)
    key_rows = draw_key_rows(jax.random.fold_in(key_of[12], 71), 0)
    value_rows = noise(key_of[2], (TOKENS, KVH * HEAD_DIM), 1.0, 6.0, ((0, 32), (1, 16)))
    sink_logits = noise(key_of[3], (QH,), 2.0, 6.0, ((0, 16),), jnp.float32)
    out_weight = noise(key_of[4], (QH * HEAD_DIM, D), (QH * HEAD_DIM) ** -0.5, 0.125, ((0, 16),))
    residual = noise(key_of[5], (TOKENS, D), 0.5, 3.0, ((0, 32),))
    norm_gain = jnp.clip(1.0 + 0.18 * jax.random.normal(key_of[6], (D,), jnp.float32), 0.1, 1.9)
    routes_keys = jax.random.split(jax.random.fold_in(key_of[7], 1), TOKENS // TOK_DEV)
    routes_turns = jax.random.permutation(jax.random.fold_in(key_of[7], 3), TOKENS // TOK_DEV)
    routes = jax.vmap(lambda own, number: deal_out(jax.random.fold_in(key_of[7], 2), own, number, TOK_DEV, EXPERTS, TOP, CAP, 1))(routes_keys, routes_turns).reshape((TOKENS, TOP))
    route_weights = jnp.clip(0.2 + 0.8 * jax.random.uniform(key_of[8], (TOKENS, TOP), jnp.float32) ** levels(key_of[8], (TOKENS, TOP), ((0, 32),), -0.2, 0.2), 0.2, 1.0)
    gate_weight = noise(key_of[9], (EXPERTS, D, FF), D ** -0.5, 0.125, ((0, 32), (2, 16)))
    up_weight = noise(key_of[10], (EXPERTS, D, FF), D ** -0.5, 0.125, ((0, 32), (2, 16)))
    down_weight = noise(key_of[11], (EXPERTS, FF, D), FF ** -0.5, 0.09375, ((0, 32), (1, 16)))
    return dict(queries=queries, key_rows=key_rows, value_rows=value_rows, sink_logits=sink_logits, out_weight=out_weight, residual=residual, norm_gain=norm_gain, routes=routes, route_weights=route_weights, gate_weight=gate_weight, up_weight=up_weight, down_weight=down_weight)


def reference(queries, key_rows, value_rows, sink_logits, out_weight, residual, norm_gain, routes, route_weights, gate_weight, up_weight, down_weight):
    blocks = TOKENS // WINDOW
    group_size = QH // KVH
    zeros_rim = jnp.zeros((WINDOW, KVH * HEAD_DIM), jnp.bfloat16)
    key_ext = jnp.concatenate([zeros_rim, key_rows], axis=0).reshape(blocks + 1, WINDOW, KVH, HEAD_DIM)
    val_ext = jnp.concatenate([zeros_rim, value_rows], axis=0).reshape(blocks + 1, WINDOW, KVH, HEAD_DIM)
    key_pair = jnp.concatenate([key_ext[:-1], key_ext[1:]], axis=1)
    val_pair = jnp.concatenate([val_ext[:-1], val_ext[1:]], axis=1)
    query_blocks = queries.reshape(blocks, WINDOW, KVH, group_size, HEAD_DIM)
    distance = jnp.arange(WINDOW)[:, None] + WINDOW - jnp.arange(2 * WINDOW)[None, :]
    key_global = jnp.arange(blocks)[:, None, None] * WINDOW + jnp.arange(2 * WINDOW)[None, None, :] - WINDOW
    allowed = (distance >= 0)[None] & (distance <= WINDOW)[None] & (key_global >= 0)
    head_ids = jnp.arange(QH)
    slopes = jnp.exp2(-8.0 * (head_ids + 1).astype(jnp.float32) / QH).reshape(KVH, group_size)

    def attend_head(inputs):
        q_head, k_head, v_head, sink_head, slope_head = inputs
        scores = jnp.einsum('bqgd,bcd->bgqc', q_head.astype(jnp.float32), k_head.astype(jnp.float32)) * HEAD_DIM ** (-0.5)
        scores = scores - slope_head[None, :, None, None] * distance.astype(jnp.float32)
        scores = jnp.where(allowed[:, None], scores, -jnp.inf)
        row_peak = lax.optimization_barrier(jnp.max(scores, axis=-1, keepdims=True))
        log_total = row_peak + jnp.log(lax.optimization_barrier(jnp.sum(jnp.exp(scores - row_peak), axis=-1, keepdims=True)))
        probs = jnp.exp(scores - log_total).astype(jnp.bfloat16)
        mixed = jnp.einsum('bgqc,bcd->bqgd', probs.astype(jnp.float32), v_head.astype(jnp.float32))
        keep_factor = jax.nn.sigmoid(log_total[..., 0] - sink_head[None, :, None])
        keep_factor = jnp.transpose(keep_factor, (0, 2, 1))[..., None]
        return (mixed * keep_factor).astype(jnp.bfloat16)
    per_head = lax.map(attend_head, (jnp.moveaxis(query_blocks, 2, 0), jnp.moveaxis(key_pair, 2, 0), jnp.moveaxis(val_pair, 2, 0), sink_logits.reshape(KVH, group_size), slopes))
    attended = jnp.moveaxis(per_head, 0, 2).reshape(TOKENS, QH * HEAD_DIM)
    columns = QH * HEAD_DIM // N_TP
    head_total = jnp.zeros((TOKENS, D), jnp.float32)
    for piece_id in range(N_TP):
        partial_value = jnp.dot(attended[:, piece_id * columns:(piece_id + 1) * columns], out_weight[piece_id * columns:(piece_id + 1) * columns], preferred_element_type=jnp.float32)
        head_total = head_total + lax.optimization_barrier(partial_value.astype(jnp.bfloat16)).astype(jnp.float32)
    mixed_state = (residual.astype(jnp.float32) + head_total).astype(jnp.bfloat16)
    state32 = mixed_state.astype(jnp.float32)
    normed = (state32 * lax.rsqrt(lax.optimization_barrier(jnp.mean(state32 * state32, axis=-1, keepdims=True)) + 1e-06) * norm_gain).astype(jnp.bfloat16)
    slots = N_SP * CAP
    flat_routes = routes.reshape(-1).astype(jnp.int32)
    token_of = (jnp.arange(TOKENS * TOP) // TOP).astype(jnp.int32)
    member = (flat_routes[:, None] == jnp.arange(EXPERTS)[None, :]).astype(jnp.int32)
    slot_rank = lax.optimization_barrier(jnp.sum((jnp.cumsum(member, axis=0) - 1) * member, axis=1)).astype(jnp.int32)

    def one_expert(inputs):
        expert_id, w_gate, w_up, w_down = inputs
        target = jnp.where(flat_routes == expert_id, slot_rank, slots).astype(jnp.int32)
        slot_token = jnp.zeros((slots,), jnp.int32).at[target].set(token_of, mode='drop')
        slot_rows = normed[slot_token]
        gate_pre = jnp.dot(slot_rows, w_gate, preferred_element_type=jnp.float32)
        up_pre = jnp.dot(slot_rows, w_up, preferred_element_type=jnp.float32)
        activated = (jax.nn.silu(gate_pre) * up_pre).astype(jnp.bfloat16)
        act_groups = activated.reshape(slots, N_TP, FF // N_TP).astype(jnp.float32)
        down_groups = w_down.reshape(N_TP, FF // N_TP, D).astype(jnp.float32)
        parts = jnp.einsum('mpf,pfd->pmd', act_groups, down_groups)
        parts = lax.optimization_barrier(parts.astype(jnp.bfloat16)).astype(jnp.float32)
        return lax.optimization_barrier(jnp.sum(parts, axis=0)).astype(jnp.bfloat16)
    outputs = lax.map(one_expert, (jnp.arange(EXPERTS, dtype=jnp.int32), gate_weight, up_weight, down_weight))
    flat_index = (flat_routes * slots + slot_rank).astype(jnp.int32)
    picked = outputs.reshape(EXPERTS * slots, D)[flat_index].reshape(TOKENS, TOP, D)
    expert_mix = lax.optimization_barrier(jnp.sum(route_weights[..., None] * picked.astype(jnp.float32), axis=1))
    return (state32 + expert_mix).astype(jnp.bfloat16)
```

```python
import functools

import jax
import jax.numpy as jnp
from jax import lax
from jax.experimental import pallas as pl
from jax.experimental.pallas import tpu as pltpu
from jax.sharding import Mesh
from jax.sharding import PartitionSpec as P

HEAD_DIM = 64
QH = 32
TOP = 2
T = 128
L = 128
G = 4
BF = jnp.bfloat16
F32 = jnp.float32
NX = 4


def dot(a, b, dims=((1,), (0,))):
    return lax.dot_general(a, b, (dims, ((), ())), preferred_element_type=F32)


def offsets(nz, nx):
    def far(k):
        dz, dx = k // nx, k % nx
        return min(dz, nz - dz) + min(dx, nx - dx)

    return [(k // nx, k % nx) for k in sorted(range(nz * nx), key=lambda k: (far(k), k))]


def layer(
    dims,
    q_ref,
    k_ref,
    v_ref,
    sink_ref,
    wo_hbm,
    res_hbm,
    gain_ref,
    routes_ref,
    rw_ref,
    wg_hbm,
    wu_hbm,
    wd_hbm,
    out_hbm,
    wo,
    wg,
    wu,
    wd,
    res,
    halo,
    p0_ref,
    p1_ref,
    pick_ref,
    own1,
    ps1,
    pr1,
    r1s,
    r1r,
    state_ref,
    disp,
    ag,
    acc_g,
    acc_u,
    ssq,
    act_ref,
    own2,
    ps2,
    pr2,
    r2s,
    r2r,
    out2,
    ret,
    fin,
    loc_sem,
    send_sem,
    halo_sem,
    p1_sem,
    r1_sem,
    disp_sem,
    agr_sem,
    agd_sem,
    p2_sem,
    r2_sem,
    ret_sem,
    fin_sem,
    find_sem,
):
    nz, nx, ny = dims
    ns = nz * nx
    slots = ns * disp.shape[1]
    cap = disp.shape[1]
    half = ny // 2
    per = ns // G
    rows = slots // G
    z, x, y, c = (lax.axis_index(a) for a in ("z", "x", "y", "c"))
    me_s = z * nx + x
    me_j = 2 * y + c
    pos = offsets(nz, nx)

    def at_y(rel):
        return lax.rem(y + (rel + ny) % ny, ny)

    def sp_at(dz, dx):
        return lax.rem(z + dz % nz, nz), lax.rem(x + dx % nx, nx)

    partner = (z, x, y, 1 - c)

    def remote(src, dst, s, r, dev):
        cp = pltpu.make_async_remote_copy(
            src_ref=src,
            dst_ref=dst,
            send_sem=s,
            recv_sem=r,
            device_id=dev,
            device_id_type=pl.DeviceIdType.MESH,
        )
        cp.start()

    def take(ref, sem):
        pltpu.make_async_copy(ref, ref, sem).wait()

    barrier = pltpu.get_barrier_semaphore()
    for dz, dx in pos[1:]:
        tz, tx = sp_at(dz, dx)
        pl.semaphore_signal(
            barrier, inc=1, device_id=(tz, tx, y, c), device_id_type=pl.DeviceIdType.MESH
        )
    for rel in range(1, ny):
        pl.semaphore_signal(
            barrier, inc=1, device_id=(z, x, at_y(rel), c), device_id_type=pl.DeviceIdType.MESH
        )
    pl.semaphore_signal(barrier, inc=1, device_id=partner, device_id_type=pl.DeviceIdType.MESH)

    def lane_block(j):
        return pl.ds(pl.multiple_of(j * L, L), L)

    pltpu.make_async_copy(res_hbm.at[:, lane_block(me_j)], res, loc_sem.at[0]).start()
    for rel in range(ny):
        for side in range(2):
            j = 2 * at_y(rel) + (c if side == 0 else 1 - c)
            pltpu.make_async_copy(
                wo_hbm.at[:, lane_block(j)], wo.at[rel, :, pl.ds(side * L, L)], loc_sem.at[1]
            ).start()
    pltpu.make_async_copy(wg_hbm.at[0], wg, loc_sem.at[2]).start()
    pltpu.make_async_copy(wu_hbm.at[0], wu, loc_sem.at[3]).start()
    for rel in range(ny):
        for side in range(2):
            j = 2 * at_y(rel) + (c if side == 0 else 1 - c)
            pltpu.make_async_copy(
                wd_hbm.at[0, :, lane_block(j)], wd.at[rel, :, pl.ds(side * L, L)], loc_sem.at[4]
            ).start()

    lanes = lax.broadcasted_iota(jnp.int32, (T, L), 1)
    subs = lax.broadcasted_iota(jnp.int32, (T, L), 0)
    chosen = routes_ref[...]
    e0, e1 = chosen[:, 0:1], chosen[:, 1:2]
    m0, m1 = e0 == lanes, e1 == lanes
    member = jnp.where(m0 | m1, 1.0, 0.0).astype(BF)
    lower = jnp.where(lanes < subs, 1.0, 0.0).astype(BF)
    before = dot(lower, member)
    rank0 = jnp.sum(jnp.where(m0, before, 0.0), axis=1, keepdims=True)
    rank1 = jnp.sum(jnp.where(m1, before, 0.0), axis=1, keepdims=True)
    slot_ids = lax.broadcasted_iota(jnp.int32, (T, slots), 1).astype(F32)
    p0 = jnp.where(slot_ids == e0.astype(F32) * cap + rank0, 1.0, 0.0)
    p1 = jnp.where(slot_ids == e1.astype(F32) * cap + rank1, 1.0, 0.0)
    p0_ref[...] = p0.astype(BF)
    p1_ref[...] = p1.astype(BF)
    pick_ref[...] = jnp.transpose(p0 + p1).astype(BF)

    dist = (subs - lanes).astype(F32)
    q = q_ref[...]
    k = k_ref[...]
    head = 2 * me_j

    def masked(h, keys, gap, allowed):
        s = dot(q[:, h * HEAD_DIM : (h + 1) * HEAD_DIM], keys, ((1,), (1,)))
        idx = jnp.full((T, L), head + h + 1, jnp.int32).astype(F32)
        slope = jnp.exp2(-8.0 * idx / QH)
        return jnp.where(allowed, s * HEAD_DIM**-0.5 - slope * gap, -1e30)

    own_s = [masked(h, k, dist, lanes <= subs) for h in range(2)]

    pl.semaphore_wait(barrier, ns + ny - 1)

    nxt = lax.rem(me_s + 1, ns)
    after = (nxt // nx, lax.rem(nxt, nx), y, c)
    remote(k_ref, halo.at[0], send_sem.at[0], halo_sem.at[0], after)
    remote(v_ref, halo.at[1], send_sem.at[1], halo_sem.at[1], after)

    take(halo.at[0], halo_sem.at[0])
    take(halo.at[1], halo_sem.at[1])
    v_own = v_ref[...]
    v_old = halo[1]
    parts = []
    for h in range(2):
        old_s = masked(h, halo[0], dist + T, (lanes >= subs) & (me_s > 0))
        peak = jnp.maximum(
            jnp.max(own_s[h], axis=1, keepdims=True), jnp.max(old_s, axis=1, keepdims=True)
        )
        total = jnp.sum(jnp.exp(own_s[h] - peak), axis=1, keepdims=True) + jnp.sum(
            jnp.exp(old_s - peak), axis=1, keepdims=True
        )
        log_total = peak + jnp.log(total)
        mixed = dot(jnp.exp(own_s[h] - log_total).astype(BF), v_own) + dot(
            jnp.exp(old_s - log_total).astype(BF), v_old
        )
        keep = 1.0 / (1.0 + jnp.exp(sink_ref[h] - log_total))
        parts.append((mixed * keep).astype(BF))
    attended = jnp.concatenate(parts, axis=1)

    rels = [half]
    for d in range(half - 1, 0, -1):
        rels += [d, ny - d]
    rels += [0]
    take(wo, loc_sem.at[1])
    for rel in rels:
        o = dot(attended, wo[rel])
        own1[rel] = o[:, :L]
        ps1[rel] = o[:, L:].astype(BF)
        remote(ps1.at[rel], pr1.at[rel], send_sem.at[2], p1_sem.at[rel], partner)
    for rel in rels[:-1]:
        take(pr1.at[rel], p1_sem.at[rel])
        r1s[rel] = (own1[rel] + pr1[rel].astype(F32)).astype(BF)
        remote(r1s.at[rel], r1r.at[rel], send_sem.at[3], r1_sem.at[rel], (z, x, at_y(rel), c))
    take(pr1.at[0], p1_sem.at[0])
    take(res, loc_sem.at[0])
    total = res[...].astype(F32) + own1[0] + pr1[0].astype(F32)
    for rel in rels[-2::-1]:
        take(r1r.at[rel], r1_sem.at[rel])
        total = total + r1r[rel].astype(F32)
    state = total.astype(BF)
    state_ref[...] = state

    disp[...] = dot(pick_ref[...], state).astype(BF).reshape(ns, cap, L)
    for p in range(1, ns):
        tz, tx = sp_at(*pos[p])
        remote(
            disp.at[tz * nx + tx],
            ag.at[me_j, p],
            send_sem.at[4],
            disp_sem.at[p // per],
            (tz, tx, y, c),
        )
    ag[me_j, 0] = disp[me_s]

    def grp(g):
        return pl.ds(g * per, per)

    def hops(way, g):
        return half if (way == 0) == (g % 2 == 0) else half - 1

    def side_of(way):
        return (z, x, at_y(1 if way == 0 else -1), c)

    def pass_on(g, way, hop, j):
        if hop < hops(way, g):
            remote(
                ag.at[j, grp(g)],
                ag.at[j, grp(g)],
                send_sem.at[5],
                agr_sem.at[way, hop, g],
                side_of(way),
            )

    def across(g, j, rel):
        remote(ag.at[j, grp(g)], ag.at[j, grp(g)], send_sem.at[6], agd_sem.at[rel], partner)

    for g in range(G):
        if g == 0:
            take(ag.at[me_j, pl.ds(1, per - 1)], disp_sem.at[0])
        else:
            take(ag.at[me_j, grp(g)], disp_sem.at[g])
        for way in range(2):
            pass_on(g, way, 0, me_j)
        across(g, me_j, 0)

    take(wg, loc_sem.at[2])
    take(wu, loc_sem.at[3])

    def absorb(rel, first=False):
        yy = at_y(rel)
        take(ag.at[2 * yy + 1 - c], agd_sem.at[rel])
        cols = pl.ds(pl.multiple_of(yy * 2 * L, 2 * L), 2 * L)
        gain = gain_ref[:, cols]
        w_g, w_u = wg[cols, :], wu[cols, :]
        for g in range(G):
            at = pl.ds(g * rows, rows)
            lo = ag[2 * yy, grp(g)].reshape(rows, L).astype(F32)
            hi = ag[2 * yy + 1, grp(g)].reshape(rows, L).astype(F32)
            lhs = jnp.concatenate(
                [(lo * gain[:, :L]).astype(BF), (hi * gain[:, L:]).astype(BF)], axis=1
            )
            square = lo * lo + hi * hi
            if first:
                ssq[at, :] = square
                acc_g[at, :] = dot(lhs, w_g)
                acc_u[at, :] = dot(lhs, w_u)
            else:
                ssq[at, :] += square
                acc_g[at, :] += dot(lhs, w_g)
                acc_u[at, :] += dot(lhs, w_u)

    for hop in range(half):
        for g in range(G):
            for way in range(2):
                if hop < hops(way, g):
                    rel = ny - hop - 1 if way == 0 else hop + 1
                    j = 2 * at_y(rel) + c
                    take(ag.at[j, grp(g)], agr_sem.at[way, hop, g])
                    pass_on(g, way, hop + 1, j)
                    across(g, j, rel)
        if hop == 0:
            absorb(0, True)
        else:
            absorb(hop)
            absorb(ny - hop)
    absorb(half)

    for g in range(G):
        at = pl.ds(g * rows, rows)
        scale = lax.rsqrt(jnp.sum(ssq[at, :], axis=1, keepdims=True) / (2 * ny * L) + 1e-06)
        gate = acc_g[at, :] * scale
        act_ref[at, :] = (gate / (1.0 + jnp.exp(-gate)) * (acc_u[at, :] * scale)).astype(BF)

    take(wd, loc_sem.at[4])
    act = act_ref[...]
    for rel in rels:
        o = dot(act, wd[rel])
        own2[rel] = o[:, :L]
        ps2[rel] = o[:, L:].astype(BF)
        remote(ps2.at[rel], pr2.at[rel], send_sem.at[7], p2_sem.at[rel], partner)

    for stage in range(half):
        rel_of = (half - stage, (ny - half + stage) % ny)
        for rel in sorted(set(rel_of)):
            take(pr2.at[rel], p2_sem.at[rel])
        for g in reversed(range(G)):
            at = pl.ds(g * rows, rows)
            for way in range(2):
                begin = half - hops(way, g)
                if stage < begin:
                    continue
                rel = rel_of[way]
                s = own2[rel, at, :] + pr2[rel, at, :].astype(F32)
                if stage > begin:
                    take(r2r.at[way, stage - 1, g], r2_sem.at[way, stage - 1, g])
                    s = s + r2r[way, stage - 1, g].astype(F32)
                r2s[way, stage, g] = s.astype(BF)
                remote(
                    r2s.at[way, stage, g],
                    r2r.at[way, stage, g],
                    send_sem.at[8],
                    r2_sem.at[way, stage, g],
                    side_of(way),
                )
    take(pr2.at[0], p2_sem.at[0])
    for g in reversed(range(G)):
        at = pl.ds(g * rows, rows)
        s = own2[0, at, :] + pr2[0, at, :].astype(F32)
        for way in range(2):
            take(r2r.at[way, half - 1, g], r2_sem.at[way, half - 1, g])
            s = s + r2r[way, half - 1, g].astype(F32)
        out2[grp(g)] = s.astype(BF).reshape(per, cap, L)
        for p in reversed(range(g * per, (g + 1) * per)):
            if p == 0:
                ret[me_s] = out2[0]
                continue
            tz, tx = sp_at(-pos[p][0], -pos[p][1])
            remote(out2.at[p], ret.at[me_s], send_sem.at[9], ret_sem.at[0], (tz, tx, y, c))

    take(ret.at[pl.ds(0, ns - 1)], ret_sem.at[0])
    back = ret[...].reshape(slots, L)
    mix = rw_ref[:, 0:1] * dot(p0_ref[...], back) + rw_ref[:, 1:2] * dot(p1_ref[...], back)
    fin[me_j] = (state_ref[...].astype(F32) + mix).astype(BF)

    def write(j):
        pltpu.make_async_copy(fin.at[j], out_hbm.at[:, lane_block(j)], loc_sem.at[5]).start()

    for rel in rels[:-1]:
        remote(fin.at[me_j], fin.at[me_j], send_sem.at[10], fin_sem.at[rel], (z, x, at_y(rel), c))
    remote(fin.at[me_j], fin.at[me_j], send_sem.at[11], find_sem.at[0], partner)
    write(me_j)
    for rel in rels[-2::-1]:
        j = 2 * at_y(-rel) + c
        take(fin.at[j], fin_sem.at[rel])
        remote(fin.at[j], fin.at[j], send_sem.at[11], find_sem.at[rel], partner)
        write(j)
    for rel in rels[::-1]:
        j = 2 * at_y(-rel) + 1 - c
        take(fin.at[j], find_sem.at[rel])
        write(j)

    take(k_ref, send_sem.at[0])
    take(v_ref, send_sem.at[1])
    take(ps1, send_sem.at[2])
    take(r1s.at[pl.ds(0, ny - 1)], send_sem.at[3])
    take(disp.at[pl.ds(0, ns - 1)], send_sem.at[4])
    take(ag.at[pl.ds(0, ny - 1)], send_sem.at[5])
    take(ag.at[pl.ds(0, ny)], send_sem.at[6])
    take(ps2, send_sem.at[7])
    take(ps2.at[pl.ds(0, ny - 1)], send_sem.at[8])
    take(out2.at[pl.ds(0, ns - 1)], send_sem.at[9])
    take(fin.at[pl.ds(0, ny - 1)], send_sem.at[10])
    take(fin.at[pl.ds(0, ny)], send_sem.at[11])
    take(out_hbm, loc_sem.at[5])


def per_device(
    dims,
    queries,
    key_rows,
    value_rows,
    sink_logits,
    out_weight,
    residual,
    norm_gain,
    routes,
    route_weights,
    gate_weight,
    up_weight,
    down_weight,
):
    nz, nx, ny = dims
    ns = nz * nx
    width = residual.shape[1]
    hidden = gate_weight.shape[2]
    cap = 2 * T * TOP // ns
    slots = ns * cap
    rows = slots // G
    half = ny // 2
    vm = pl.BlockSpec(memory_space=pltpu.VMEM)
    hbm = pl.BlockSpec(memory_space=pl.ANY)
    sm = pl.BlockSpec(memory_space=pltpu.SMEM)
    scratch = [
        pltpu.VMEM((ny, T, 2 * L), BF),
        pltpu.VMEM((width, hidden), BF),
        pltpu.VMEM((width, hidden), BF),
        pltpu.VMEM((ny, hidden, 2 * L), BF),
        pltpu.VMEM((T, L), BF),
        pltpu.VMEM((2, T, HEAD_DIM), BF),
        pltpu.VMEM((T, slots), BF),
        pltpu.VMEM((T, slots), BF),
        pltpu.VMEM((slots, T), BF),
        pltpu.VMEM((ny, T, L), F32),
        pltpu.VMEM((ny, T, L), BF),
        pltpu.VMEM((ny, T, L), BF),
        pltpu.VMEM((ny, T, L), BF),
        pltpu.VMEM((ny, T, L), BF),
        pltpu.VMEM((T, L), BF),
        pltpu.VMEM((ns, cap, L), BF),
        pltpu.VMEM((2 * ny, ns, cap, L), BF),
        pltpu.VMEM((slots, hidden), F32),
        pltpu.VMEM((slots, hidden), F32),
        pltpu.VMEM((slots, L), F32),
        pltpu.VMEM((slots, hidden), BF),
        pltpu.VMEM((ny, slots, L), F32),
        pltpu.VMEM((ny, slots, L), BF),
        pltpu.VMEM((ny, slots, L), BF),
        pltpu.VMEM((2, half, G, rows, L), BF),
        pltpu.VMEM((2, half, G, rows, L), BF),
        pltpu.VMEM((ns, cap, L), BF),
        pltpu.VMEM((ns, cap, L), BF),
        pltpu.VMEM((2 * ny, T, L), BF),
        pltpu.SemaphoreType.DMA((6,)),
        pltpu.SemaphoreType.DMA((12,)),
        pltpu.SemaphoreType.DMA((2,)),
        pltpu.SemaphoreType.DMA((ny,)),
        pltpu.SemaphoreType.DMA((ny,)),
        pltpu.SemaphoreType.DMA((G,)),
        pltpu.SemaphoreType.DMA((2, half, G)),
        pltpu.SemaphoreType.DMA((ny,)),
        pltpu.SemaphoreType.DMA((ny,)),
        pltpu.SemaphoreType.DMA((2, half, G)),
        pltpu.SemaphoreType.DMA((1,)),
        pltpu.SemaphoreType.DMA((ny,)),
        pltpu.SemaphoreType.DMA((ny,)),
    ]
    return pl.pallas_call(
        functools.partial(layer, dims),
        out_shape=jax.ShapeDtypeStruct((T, width), BF),
        in_specs=[vm, vm, vm, sm, hbm, hbm, vm, vm, vm, hbm, hbm, hbm],
        out_specs=hbm,
        scratch_shapes=scratch,
        compiler_params=pltpu.CompilerParams(
            collective_id=0, has_side_effects=True, vmem_limit_bytes=48 * 1024 * 1024
        ),
        name="layer",
    )(
        queries,
        key_rows,
        value_rows,
        sink_logits,
        out_weight,
        residual,
        norm_gain.reshape(1, width),
        routes,
        route_weights,
        gate_weight,
        up_weight,
        down_weight,
    )


def build(devices, dims):
    torus = Mesh(devices.reshape(*dims, 2), ("z", "x", "y", "c"))
    sp, tp = ("z", "x"), ("y", "c")
    placed = (
        P(sp, tp),
        P(sp, tp),
        P(sp, tp),
        P(tp),
        P(tp, None),
        P(sp, None),
        P(),
        P(sp, None),
        P(sp, None),
        P(sp, None, tp),
        P(sp, None, tp),
        P(sp, tp, None),
    )
    return jax.shard_map(
        functools.partial(per_device, dims),
        mesh=torus,
        in_specs=placed,
        out_specs=P(sp, None),
        check_vma=False,
    )


def solution(mesh):
    sp, tp = mesh.shape["sp"], mesh.shape["tp"]
    return build(mesh.devices, (sp // NX, NX, tp // 2))
```

```python
import functools

import jax
import jax.numpy as jnp
from jax import lax
from jax.experimental import pallas as pl
from jax.experimental.pallas import tpu as pltpu
from jax.sharding import Mesh
from jax.sharding import PartitionSpec as P

HEAD_DIM = 64
QH = 32
TOP = 2
T = 128
L = 128
G = 4
BF = jnp.bfloat16
F32 = jnp.float32
NX = 4


def dot(a, b, dims=((1,), (0,))):
    return lax.dot_general(a, b, (dims, ((), ())), preferred_element_type=F32)


def offsets(nz, nx):
    def far(k):
        dz, dx = k // nx, k % nx
        return min(dz, nz - dz) + min(dx, nx - dx)

    return [(k // nx, k % nx) for k in sorted(range(nz * nx), key=lambda k: (far(k), k))]


def layer(
    dims,
    q_hbm,
    k_hbm,
    v_hbm,
    sink_ref,
    wo_hbm,
    res_hbm,
    gain_hbm,
    routes_hbm,
    rw_hbm,
    wg_hbm,
    wu_hbm,
    wd_hbm,
    out_hbm,
    q_ref,
    kv_ref,
    gain_ref,
    routes_ref,
    rw_ref,
    rate_ref,
    wo,
    wg,
    wu,
    wd,
    res,
    halo,
    p0_ref,
    p1_ref,
    pick_ref,
    own1,
    ps1,
    pr1,
    r1s,
    r1r,
    state_ref,
    disp,
    ag,
    acc_g,
    acc_u,
    ssq,
    act_ref,
    own2,
    ps2,
    pr2,
    r2s,
    r2r,
    out2,
    ret,
    fin,
    loc_sem,
    send_sem,
    halo_sem,
    p1_sem,
    r1_sem,
    disp_sem,
    agr_sem,
    agd_sem,
    p2_sem,
    r2_sem,
    ret_sem,
    fin_sem,
    find_sem,
):
    nz, nx, ny = dims
    ns = nz * nx
    slots = ns * disp.shape[1]
    cap = disp.shape[1]
    half = ny // 2
    per = ns // G
    rows = slots // G
    z, x, y, c = (lax.axis_index(a) for a in ("z", "x", "y", "c"))
    me_s = z * nx + x
    me_j = 2 * y + c
    pos = offsets(nz, nx)

    def at_y(rel):
        return lax.rem(y + (rel + ny) % ny, ny)

    def sp_at(dz, dx):
        return lax.rem(z + dz % nz, nz), lax.rem(x + dx % nx, nx)

    partner = (z, x, y, 1 - c)

    def remote(src, dst, s, r, dev):
        cp = pltpu.make_async_remote_copy(
            src_ref=src,
            dst_ref=dst,
            send_sem=s,
            recv_sem=r,
            device_id=dev,
            device_id_type=pl.DeviceIdType.MESH,
        )
        cp.start()

    def take(ref, sem):
        pltpu.make_async_copy(ref, ref, sem).wait()

    barrier = pltpu.get_barrier_semaphore()
    for dz, dx in pos[1:]:
        tz, tx = sp_at(dz, dx)
        pl.semaphore_signal(
            barrier, inc=1, device_id=(tz, tx, y, c), device_id_type=pl.DeviceIdType.MESH
        )
    for rel in range(1, ny):
        pl.semaphore_signal(
            barrier, inc=1, device_id=(z, x, at_y(rel), c), device_id_type=pl.DeviceIdType.MESH
        )
    pl.semaphore_signal(barrier, inc=1, device_id=partner, device_id_type=pl.DeviceIdType.MESH)

    def lane_block(j):
        return pl.ds(pl.multiple_of(j * L, L), L)

    loads = {}

    def load(name, src, dst, sem):
        pltpu.make_async_copy(src, dst, loc_sem.at[sem]).start()
        loads[name] = (dst, loc_sem.at[sem])

    def ready(name):
        take(*loads.pop(name))

    pending = []

    load("k", k_hbm, kv_ref.at[0], 6)
    load("v", v_hbm, kv_ref.at[1], 7)
    load("q", q_hbm, q_ref, 8)
    load("routes", routes_hbm, routes_ref, 9)
    load("rw", rw_hbm, rw_ref, 10)
    load("gain", gain_hbm, gain_ref, 11)
    load("res", res_hbm.at[:, lane_block(me_j)], res, 0)
    for rel in range(ny):
        for side in range(2):
            j = 2 * at_y(rel) + (c if side == 0 else 1 - c)
            pltpu.make_async_copy(
                wo_hbm.at[:, lane_block(j)], wo.at[rel, :, pl.ds(side * L, L)], loc_sem.at[1]
            ).start()
    loads["wo"] = (wo, loc_sem.at[1])
    load("wg", wg_hbm.at[0], wg, 2)
    load("wu", wu_hbm.at[0], wu, 3)
    for rel in range(ny):
        for side in range(2):
            j = 2 * at_y(rel) + (c if side == 0 else 1 - c)
            pltpu.make_async_copy(
                wd_hbm.at[0, :, lane_block(j)], wd.at[rel, :, pl.ds(side * L, L)], loc_sem.at[4]
            ).start()
    loads["wd"] = (wd, loc_sem.at[4])

    ready("routes")
    ready("rw")
    lanes = lax.broadcasted_iota(jnp.int32, (T, L), 1)
    subs = lax.broadcasted_iota(jnp.int32, (T, L), 0)
    experts = lax.broadcasted_iota(jnp.int32, (ns, T), 0)
    slot_ids = lax.broadcasted_iota(jnp.int32, (slots, T), 0).astype(F32)
    earlier = jnp.where(subs < lanes, 1.0, 0.0).astype(BF)
    chosen = [routes_ref[t : t + 1, :] for t in range(TOP)]
    named = [e == experts for e in chosen]
    member = jnp.where(named[0] | named[1], 1.0, 0.0).astype(BF)
    before = dot(member, earlier)
    picks = []
    for t in range(TOP):
        rank = jnp.sum(jnp.where(named[t], before, 0.0), axis=0, keepdims=True)
        picks.append(jnp.where(slot_ids == chosen[t].astype(F32) * cap + rank, 1.0, 0.0))
        rate_ref[t] = jnp.transpose(jnp.broadcast_to(rw_ref[t : t + 1, :], (L, T)))
    p0_ref[...] = jnp.transpose(picks[0]).astype(BF)
    p1_ref[...] = jnp.transpose(picks[1]).astype(BF)
    pick_ref[...] = (picks[0] + picks[1]).astype(BF)

    dist = (subs - lanes).astype(F32)
    ready("q")
    ready("k")
    ready("v")
    q = q_ref[...]
    head = 2 * me_j

    def masked(h, keys, gap, allowed):
        s = dot(q[:, h * HEAD_DIM : (h + 1) * HEAD_DIM], keys)
        idx = jnp.full((T, L), head + h + 1, jnp.int32).astype(F32)
        slope = jnp.exp2(-8.0 * idx / QH)
        return jnp.where(allowed, s * HEAD_DIM**-0.5 - slope * gap, -1e30)

    own_s = [masked(h, kv_ref[0], dist, lanes <= subs) for h in range(2)]

    pl.semaphore_wait(barrier, ns + ny - 1)

    nxt = lax.rem(me_s + 1, ns)
    after = (nxt // nx, lax.rem(nxt, nx), y, c)
    remote(kv_ref, halo, send_sem.at[0], halo_sem.at[0], after)
    pending.append((kv_ref, send_sem.at[0]))
    take(halo, halo_sem.at[0])
    v_own = kv_ref[1]
    v_old = halo[1]
    parts = []
    for h in range(2):
        old_s = masked(h, halo[0], dist + T, (lanes >= subs) & (me_s > 0))
        peak = jnp.maximum(
            jnp.max(own_s[h], axis=1, keepdims=True), jnp.max(old_s, axis=1, keepdims=True)
        )
        total = jnp.sum(jnp.exp(own_s[h] - peak), axis=1, keepdims=True) + jnp.sum(
            jnp.exp(old_s - peak), axis=1, keepdims=True
        )
        log_total = peak + jnp.log(total)
        mixed = dot(jnp.exp(own_s[h] - log_total).astype(BF), v_own, ((1,), (1,))) + dot(
            jnp.exp(old_s - log_total).astype(BF), v_old, ((1,), (1,))
        )
        keep = 1.0 / (1.0 + jnp.exp(sink_ref[h] - log_total))
        parts.append((mixed * keep).astype(BF))
    attended = jnp.concatenate(parts, axis=1)

    rels = [half]
    for d in range(half - 1, 0, -1):
        rels += [d, ny - d]
    rels += [0]
    ready("wo")
    for rel in rels:
        o = dot(attended, wo[rel])
        own1[rel] = o[:, :L]
        ps1[rel] = o[:, L:].astype(BF)
        remote(ps1.at[rel], pr1.at[rel], send_sem.at[2], p1_sem.at[rel], partner)
    pending.append((ps1, send_sem.at[2]))
    for rel in rels[:-1]:
        take(pr1.at[rel], p1_sem.at[rel])
        r1s[rel] = (own1[rel] + pr1[rel].astype(F32)).astype(BF)
        remote(r1s.at[rel], r1r.at[rel], send_sem.at[3], r1_sem.at[rel], (z, x, at_y(rel), c))
    pending.append((r1s.at[pl.ds(0, ny - 1)], send_sem.at[3]))
    take(pr1.at[0], p1_sem.at[0])
    ready("res")
    total = res[...].astype(F32) + own1[0] + pr1[0].astype(F32)
    for rel in rels[-2::-1]:
        take(r1r.at[rel], r1_sem.at[rel])
        total = total + r1r[rel].astype(F32)
    state = total.astype(BF)
    state_ref[...] = state

    disp[...] = dot(pick_ref[...], state).astype(BF).reshape(ns, cap, L)
    for p in range(1, ns):
        tz, tx = sp_at(*pos[p])
        remote(
            disp.at[tz * nx + tx],
            ag.at[me_j, p],
            send_sem.at[4],
            disp_sem.at[p // per],
            (tz, tx, y, c),
        )
    ag[me_j, 0] = disp[me_s]
    pending.append((disp.at[pl.ds(0, ns - 1)], send_sem.at[4]))

    def grp(g):
        return pl.ds(g * per, per)

    def hops(way, g):
        return half if (way == 0) == (g % 2 == 0) else half - 1

    def side_of(way):
        return (z, x, at_y(1 if way == 0 else -1), c)

    def pass_on(g, way, hop, j):
        if hop < hops(way, g):
            remote(
                ag.at[j, grp(g)],
                ag.at[j, grp(g)],
                send_sem.at[5],
                agr_sem.at[way, hop, g],
                side_of(way),
            )

    def across(g, j, rel):
        remote(ag.at[j, grp(g)], ag.at[j, grp(g)], send_sem.at[6], agd_sem.at[rel], partner)

    for g in range(G):
        if g == 0:
            take(ag.at[me_j, pl.ds(1, per - 1)], disp_sem.at[0])
        else:
            take(ag.at[me_j, grp(g)], disp_sem.at[g])
        for way in range(2):
            pass_on(g, way, 0, me_j)
        across(g, me_j, 0)

    ready("wg")
    ready("wu")
    ready("gain")

    def absorb(rel, first=False):
        yy = at_y(rel)
        take(ag.at[2 * yy + 1 - c], agd_sem.at[rel])
        cols = pl.ds(pl.multiple_of(yy * 2 * L, 2 * L), 2 * L)
        gain = gain_ref[:, cols]
        w_g, w_u = wg[cols, :], wu[cols, :]
        for g in range(G):
            at = pl.ds(g * rows, rows)
            lo = ag[2 * yy, grp(g)].reshape(rows, L).astype(F32)
            hi = ag[2 * yy + 1, grp(g)].reshape(rows, L).astype(F32)
            lhs = jnp.concatenate(
                [(lo * gain[:, :L]).astype(BF), (hi * gain[:, L:]).astype(BF)], axis=1
            )
            square = lo * lo + hi * hi
            if first:
                ssq[at, :] = square
                acc_g[at, :] = dot(lhs, w_g)
                acc_u[at, :] = dot(lhs, w_u)
            else:
                ssq[at, :] += square
                acc_g[at, :] += dot(lhs, w_g)
                acc_u[at, :] += dot(lhs, w_u)

    for hop in range(half):
        for g in range(G):
            for way in range(2):
                if hop < hops(way, g):
                    rel = ny - hop - 1 if way == 0 else hop + 1
                    j = 2 * at_y(rel) + c
                    take(ag.at[j, grp(g)], agr_sem.at[way, hop, g])
                    pass_on(g, way, hop + 1, j)
                    across(g, j, rel)
        if hop == 0:
            absorb(0, True)
        else:
            absorb(hop)
            absorb(ny - hop)
    absorb(half)
    pending.append((ag.at[pl.ds(0, ny - 1)], send_sem.at[5]))
    pending.append((ag.at[pl.ds(0, ny)], send_sem.at[6]))

    for g in range(G):
        at = pl.ds(g * rows, rows)
        scale = lax.rsqrt(jnp.sum(ssq[at, :], axis=1, keepdims=True) / (2 * ny * L) + 1e-06)
        gate = acc_g[at, :] * scale
        act_ref[at, :] = (gate / (1.0 + jnp.exp(-gate)) * (acc_u[at, :] * scale)).astype(BF)

    ready("wd")
    act = act_ref[...]
    for rel in rels:
        o = dot(act, wd[rel])
        own2[rel] = o[:, :L]
        ps2[rel] = o[:, L:].astype(BF)
        remote(ps2.at[rel], pr2.at[rel], send_sem.at[7], p2_sem.at[rel], partner)

    pending.append((ps2, send_sem.at[7]))
    for stage in range(half):
        rel_of = (half - stage, (ny - half + stage) % ny)
        for rel in sorted(set(rel_of)):
            take(pr2.at[rel], p2_sem.at[rel])
        for g in reversed(range(G)):
            at = pl.ds(g * rows, rows)
            for way in range(2):
                begin = half - hops(way, g)
                if stage < begin:
                    continue
                rel = rel_of[way]
                s = own2[rel, at, :] + pr2[rel, at, :].astype(F32)
                if stage > begin:
                    take(r2r.at[way, stage - 1, g], r2_sem.at[way, stage - 1, g])
                    s = s + r2r[way, stage - 1, g].astype(F32)
                r2s[way, stage, g] = s.astype(BF)
                remote(
                    r2s.at[way, stage, g],
                    r2r.at[way, stage, g],
                    send_sem.at[8],
                    r2_sem.at[way, stage, g],
                    side_of(way),
                )
    take(pr2.at[0], p2_sem.at[0])
    for g in reversed(range(G)):
        at = pl.ds(g * rows, rows)
        s = own2[0, at, :] + pr2[0, at, :].astype(F32)
        for way in range(2):
            take(r2r.at[way, half - 1, g], r2_sem.at[way, half - 1, g])
            s = s + r2r[way, half - 1, g].astype(F32)
        out2[grp(g)] = s.astype(BF).reshape(per, cap, L)
        for p in reversed(range(g * per, (g + 1) * per)):
            if p == 0:
                ret[me_s] = out2[0]
                continue
            tz, tx = sp_at(-pos[p][0], -pos[p][1])
            remote(out2.at[p], ret.at[me_s], send_sem.at[9], ret_sem.at[0], (tz, tx, y, c))

    pending.append((ps2.at[pl.ds(0, ny - 1)], send_sem.at[8]))
    pending.append((out2.at[pl.ds(0, ns - 1)], send_sem.at[9]))
    take(ret.at[pl.ds(0, ns - 1)], ret_sem.at[0])
    back = ret[...].reshape(slots, L)
    mix = rate_ref[0] * dot(p0_ref[...], back) + rate_ref[1] * dot(p1_ref[...], back)
    fin[me_j] = (state_ref[...].astype(F32) + mix).astype(BF)

    def write(j):
        pltpu.make_async_copy(fin.at[j], out_hbm.at[:, lane_block(j)], loc_sem.at[5]).start()

    for rel in rels[:-1]:
        remote(fin.at[me_j], fin.at[me_j], send_sem.at[10], fin_sem.at[rel], (z, x, at_y(rel), c))
    remote(fin.at[me_j], fin.at[me_j], send_sem.at[11], find_sem.at[0], partner)
    write(me_j)
    for rel in rels[-2::-1]:
        j = 2 * at_y(-rel) + c
        take(fin.at[j], fin_sem.at[rel])
        remote(fin.at[j], fin.at[j], send_sem.at[11], find_sem.at[rel], partner)
        write(j)
    for rel in rels[::-1]:
        j = 2 * at_y(-rel) + 1 - c
        take(fin.at[j], find_sem.at[rel])
        write(j)

    pending.append((fin.at[pl.ds(0, ny - 1)], send_sem.at[10]))
    pending.append((fin.at[pl.ds(0, ny)], send_sem.at[11]))
    pending.append((out_hbm, loc_sem.at[5]))
    for ref, sem in pending:
        take(ref, sem)


def per_device(
    dims,
    queries,
    key_rows,
    value_rows,
    sink_logits,
    out_weight,
    residual,
    norm_gain,
    routes,
    route_weights,
    gate_weight,
    up_weight,
    down_weight,
):
    nz, nx, ny = dims
    ns = nz * nx
    width = residual.shape[1]
    hidden = gate_weight.shape[2]
    cap = 2 * T * TOP // ns
    slots = ns * cap
    rows = slots // G
    half = ny // 2
    hbm = pl.BlockSpec(memory_space=pl.ANY)
    sm = pl.BlockSpec(memory_space=pltpu.SMEM)
    scratch = [
        pltpu.VMEM((T, L), BF),
        pltpu.VMEM((2, HEAD_DIM, T), BF),
        pltpu.VMEM((1, width), F32),
        pltpu.VMEM((TOP, T), jnp.int32),
        pltpu.VMEM((TOP, T), F32),
        pltpu.VMEM((TOP, T, L), F32),
        pltpu.VMEM((ny, T, 2 * L), BF),
        pltpu.VMEM((width, hidden), BF),
        pltpu.VMEM((width, hidden), BF),
        pltpu.VMEM((ny, hidden, 2 * L), BF),
        pltpu.VMEM((T, L), BF),
        pltpu.VMEM((2, HEAD_DIM, T), BF),
        pltpu.VMEM((T, slots), BF),
        pltpu.VMEM((T, slots), BF),
        pltpu.VMEM((slots, T), BF),
        pltpu.VMEM((ny, T, L), F32),
        pltpu.VMEM((ny, T, L), BF),
        pltpu.VMEM((ny, T, L), BF),
        pltpu.VMEM((ny, T, L), BF),
        pltpu.VMEM((ny, T, L), BF),
        pltpu.VMEM((T, L), BF),
        pltpu.VMEM((ns, cap, L), BF),
        pltpu.VMEM((2 * ny, ns, cap, L), BF),
        pltpu.VMEM((slots, hidden), F32),
        pltpu.VMEM((slots, hidden), F32),
        pltpu.VMEM((slots, L), F32),
        pltpu.VMEM((slots, hidden), BF),
        pltpu.VMEM((ny, slots, L), F32),
        pltpu.VMEM((ny, slots, L), BF),
        pltpu.VMEM((ny, slots, L), BF),
        pltpu.VMEM((2, half, G, rows, L), BF),
        pltpu.VMEM((2, half, G, rows, L), BF),
        pltpu.VMEM((ns, cap, L), BF),
        pltpu.VMEM((ns, cap, L), BF),
        pltpu.VMEM((2 * ny, T, L), BF),
        pltpu.SemaphoreType.DMA((12,)),
        pltpu.SemaphoreType.DMA((12,)),
        pltpu.SemaphoreType.DMA((1,)),
        pltpu.SemaphoreType.DMA((ny,)),
        pltpu.SemaphoreType.DMA((ny,)),
        pltpu.SemaphoreType.DMA((G,)),
        pltpu.SemaphoreType.DMA((2, half, G)),
        pltpu.SemaphoreType.DMA((ny,)),
        pltpu.SemaphoreType.DMA((ny,)),
        pltpu.SemaphoreType.DMA((2, half, G)),
        pltpu.SemaphoreType.DMA((1,)),
        pltpu.SemaphoreType.DMA((ny,)),
        pltpu.SemaphoreType.DMA((ny,)),
    ]
    return pl.pallas_call(
        functools.partial(layer, dims),
        out_shape=jax.ShapeDtypeStruct((T, width), BF),
        in_specs=[hbm, hbm, hbm, sm] + [hbm] * 8,
        out_specs=hbm,
        scratch_shapes=scratch,
        compiler_params=pltpu.CompilerParams(
            collective_id=0, has_side_effects=True, vmem_limit_bytes=67043328
        ),
        name="layer",
    )(
        queries,
        key_rows.T,
        value_rows.T,
        sink_logits,
        out_weight,
        residual,
        norm_gain.reshape(1, width),
        routes.T,
        route_weights.T,
        gate_weight,
        up_weight,
        down_weight,
    )


def build(devices, dims):
    torus = Mesh(devices.reshape(*dims, 2), ("z", "x", "y", "c"))
    sp, tp = ("z", "x"), ("y", "c")
    placed = (
        P(sp, tp),
        P(sp, tp),
        P(sp, tp),
        P(tp),
        P(tp, None),
        P(sp, None),
        P(),
        P(sp, None),
        P(sp, None),
        P(sp, None, tp),
        P(sp, None, tp),
        P(sp, tp, None),
    )
    return jax.shard_map(
        functools.partial(per_device, dims),
        mesh=torus,
        in_specs=placed,
        out_specs=P(sp, None),
        check_vma=False,
    )


def solution(mesh):
    sp, tp = mesh.shape["sp"], mesh.shape["tp"]
    return build(mesh.devices, (sp // NX, NX, tp // 2))
```

```python
import functools

import jax
import jax.numpy as jnp
from jax import lax
from jax.experimental import pallas as pl
from jax.experimental.pallas import tpu as pltpu
from jax.sharding import Mesh
from jax.sharding import PartitionSpec as P

HEAD_DIM = 64
QH = 32
TOP = 2
T = 128
L = 128
G = 8
HS = 2
BF = jnp.bfloat16
F32 = jnp.float32
NX = 4


def dot(a, b, dims=((1,), (0,))):
    return lax.dot_general(a, b, (dims, ((), ())), preferred_element_type=F32)


def offsets(nz, nx):
    def far(k):
        dz, dx = k // nx, k % nx
        return min(dz, nz - dz) + min(dx, nx - dx)

    return [(k // nx, k % nx) for k in sorted(range(nz * nx), key=lambda k: (far(k), k))]


def layer(
    dims,
    q_hbm,
    k_hbm,
    v_hbm,
    sink_ref,
    wo_hbm,
    res_hbm,
    gain_hbm,
    routes_hbm,
    rw_hbm,
    wg_hbm,
    wu_hbm,
    wd_hbm,
    out_hbm,
    q_ref,
    kv_ref,
    gain_ref,
    routes_ref,
    rw_ref,
    rate_ref,
    wo,
    wg,
    wu,
    wd,
    res,
    halo,
    old_ref,
    p0_ref,
    p1_ref,
    pick_ref,
    own1,
    ps1,
    pr1,
    r1s,
    r1r,
    state_ref,
    disp,
    ag,
    acc_g,
    acc_u,
    ssq,
    act_ref,
    own2,
    ps2,
    pr2,
    r2s,
    r2r,
    out2,
    ret,
    fin,
    loc_sem,
    send_sem,
    halo_sem,
    p1_sem,
    r1_sem,
    disp_sem,
    agr_sem,
    agd_sem,
    p2_sem,
    r2_sem,
    ret_sem,
    fin_sem,
    find_sem,
    know_sem,
):
    nz, nx, ny = dims
    ns = nz * nx
    slots = ns * disp.shape[1]
    cap = disp.shape[1]
    half = ny // 2
    per = ns // G
    rows = slots // G
    z, x, y, c = (lax.axis_index(a) for a in ("z", "x", "y", "c"))
    me_s = z * nx + x
    me_j = 2 * y + c
    pos = offsets(nz, nx)

    def at_y(rel):
        return lax.rem(y + (rel + ny) % ny, ny)

    def sp_at(dz, dx):
        return lax.rem(z + dz % nz, nz), lax.rem(x + dx % nx, nx)

    partner = (z, x, y, 1 - c)

    def remote(src, dst, s, r, dev):
        cp = pltpu.make_async_remote_copy(
            src_ref=src,
            dst_ref=dst,
            send_sem=s,
            recv_sem=r,
            device_id=dev,
            device_id_type=pl.DeviceIdType.MESH,
        )
        cp.start()

    def take(ref, sem):
        pltpu.make_async_copy(ref, ref, sem).wait()

    barrier = pltpu.get_barrier_semaphore()

    def along(d):
        at = lax.rem(me_s + d + ns, ns)
        return at // nx, lax.rem(at, nx), y, c

    def signal(sem, dev):
        pl.semaphore_signal(sem, inc=1, device_id=dev, device_id_type=pl.DeviceIdType.MESH)

    signal(barrier, along(1))
    signal(barrier, along(-1))
    signal(barrier, partner)
    for rel in range(1, ny):
        signal(barrier, (z, x, at_y(rel), c))
    shifts = [1 << i for i in range(know_sem.shape[0])]

    def tell(i):
        signal(know_sem.at[i], along(shifts[i]))
        signal(know_sem.at[i], along(-shifts[i]))

    def hear(i):
        pl.semaphore_wait(know_sem.at[i], 2)
        if i + 1 < len(shifts):
            tell(i + 1)

    heard = iter(range(len(shifts)))

    def hear_next():
        for i in heard:
            hear(i)
            return

    def lane_block(j):
        return pl.ds(pl.multiple_of(j * L, L), L)

    loads = {}

    def load(name, src, dst, sem):
        pltpu.make_async_copy(src, dst, loc_sem.at[sem]).start()
        loads[name] = (dst, loc_sem.at[sem])

    def ready(name):
        take(*loads.pop(name))

    pending = []

    load("k", k_hbm, kv_ref.at[0], 6)
    load("v", v_hbm, kv_ref.at[1], 7)
    load("q", q_hbm, q_ref, 8)
    load("routes", routes_hbm, routes_ref, 9)
    load("rw", rw_hbm, rw_ref, 10)
    load("gain", gain_hbm, gain_ref, 11)
    load("res", res_hbm.at[:, lane_block(me_j)], res, 0)
    for rel in range(ny):
        for side in range(2):
            j = 2 * at_y(rel) + (c if side == 0 else 1 - c)
            pltpu.make_async_copy(
                wo_hbm.at[:, lane_block(j)], wo.at[rel, :, pl.ds(side * L, L)], loc_sem.at[1]
            ).start()
    loads["wo"] = (wo, loc_sem.at[1])
    load("wg", wg_hbm.at[0], wg, 2)
    load("wu", wu_hbm.at[0], wu, 3)
    for rel in range(ny):
        for side in range(2):
            j = 2 * at_y(rel) + (c if side == 0 else 1 - c)
            pltpu.make_async_copy(
                wd_hbm.at[0, :, lane_block(j)], wd.at[rel, :, pl.ds(side * L, L)], loc_sem.at[4]
            ).start()
    loads["wd"] = (wd, loc_sem.at[4])

    ready("routes")
    ready("rw")
    lanes = lax.broadcasted_iota(jnp.int32, (T, L), 1)
    subs = lax.broadcasted_iota(jnp.int32, (T, L), 0)
    experts = lax.broadcasted_iota(jnp.int32, (ns, T), 0)
    slot_ids = lax.broadcasted_iota(jnp.int32, (slots, T), 0).astype(F32)
    earlier = jnp.where(subs < lanes, 1.0, 0.0).astype(BF)
    chosen = [routes_ref[t : t + 1, :] for t in range(TOP)]
    named = [e == experts for e in chosen]
    member = jnp.where(named[0] | named[1], 1.0, 0.0).astype(BF)
    before = dot(member, earlier)
    picks = []
    for t in range(TOP):
        rank = jnp.sum(jnp.where(named[t], before, 0.0), axis=0, keepdims=True)
        picks.append(jnp.where(slot_ids == chosen[t].astype(F32) * cap + rank, 1.0, 0.0))
        rate_ref[t] = jnp.transpose(jnp.broadcast_to(rw_ref[t : t + 1, :], (L, T)))
    p0_ref[...] = jnp.transpose(picks[0]).astype(BF)
    p1_ref[...] = jnp.transpose(picks[1]).astype(BF)
    pick_ref[...] = (picks[0] + picks[1]).astype(BF)

    dist = (subs - lanes).astype(F32)
    ready("q")
    ready("k")
    ready("v")
    q = q_ref[...]
    head = 2 * me_j

    def masked(h, keys, gap, allowed):
        s = dot(q[:, h * HEAD_DIM : (h + 1) * HEAD_DIM], keys)
        idx = jnp.full((T, L), head + h + 1, jnp.int32).astype(F32)
        slope = jnp.exp2(-8.0 * idx / QH)
        return jnp.where(allowed, s * HEAD_DIM**-0.5 - slope * gap, -1e30)

    own_s = [masked(h, kv_ref[0], dist, lanes <= subs) for h in range(2)]

    pl.semaphore_wait(barrier, ny + 2)
    tell(0)

    @pl.when(me_s < ns - 1)
    def _():
        remote(kv_ref, halo, send_sem.at[0], halo_sem.at[0], along(1))

    @pl.when(me_s > 0)
    def _():
        take(halo, halo_sem.at[0])
        old_ref[...] = halo[...]

    @pl.when(me_s == 0)
    def _():
        old_ref[...] = kv_ref[...]

    v_own = kv_ref[1]
    k_old = old_ref[0]
    v_old = old_ref[1]
    parts = []
    for h in range(2):
        old_s = masked(h, k_old, dist + T, (lanes >= subs) & (me_s > 0))
        peak = jnp.maximum(
            jnp.max(own_s[h], axis=1, keepdims=True), jnp.max(old_s, axis=1, keepdims=True)
        )
        total = jnp.sum(jnp.exp(own_s[h] - peak), axis=1, keepdims=True) + jnp.sum(
            jnp.exp(old_s - peak), axis=1, keepdims=True
        )
        log_total = peak + jnp.log(total)
        mixed = dot(jnp.exp(own_s[h] - log_total).astype(BF), v_own, ((1,), (1,))) + dot(
            jnp.exp(old_s - log_total).astype(BF), v_old, ((1,), (1,))
        )
        keep = 1.0 / (1.0 + jnp.exp(sink_ref[h] - log_total))
        parts.append((mixed * keep).astype(BF))
    attended = jnp.concatenate(parts, axis=1)

    rels = [half]
    for d in range(half - 1, 0, -1):
        rels += [d, ny - d]
    rels += [0]
    ready("wo")
    for rel in rels:
        o = dot(attended, wo[rel])
        own1[rel] = o[:, :L]
        ps1[rel] = o[:, L:].astype(BF)
        remote(ps1.at[rel], pr1.at[rel], send_sem.at[2], p1_sem.at[rel], partner)
    pending.append((ps1, send_sem.at[2]))
    hear_next()
    for rel in rels[:-1]:
        take(pr1.at[rel], p1_sem.at[rel])
        r1s[rel] = (own1[rel] + pr1[rel].astype(F32)).astype(BF)
        remote(r1s.at[rel], r1r.at[rel], send_sem.at[3], r1_sem.at[rel], (z, x, at_y(rel), c))
    pending.append((r1s.at[pl.ds(0, ny - 1)], send_sem.at[3]))
    hear_next()
    take(pr1.at[0], p1_sem.at[0])
    ready("res")
    total = res[...].astype(F32) + own1[0] + pr1[0].astype(F32)
    for i, rel in enumerate(rels[-2::-1]):
        take(r1r.at[rel], r1_sem.at[rel])
        total = total + r1r[rel].astype(F32)
        if i == half:
            hear_next()
    state = total.astype(BF)
    state_ref[...] = state

    for i in heard:
        hear(i)
    disp[...] = dot(pick_ref[...], state).astype(BF).reshape(ns, cap, L)
    for p in range(1, ns):
        tz, tx = sp_at(*pos[p])
        remote(
            disp.at[tz * nx + tx],
            ag.at[me_j, p],
            send_sem.at[4],
            disp_sem.at[p // per],
            (tz, tx, y, c),
        )
    ag[me_j, 0] = disp[me_s]
    pending.append((disp.at[pl.ds(0, ns - 1)], send_sem.at[4]))

    def grp(g):
        return pl.ds(g * per, per)

    def hops(way, g):
        return half if (way == 0) == (g % 2 == 0) else half - 1

    def side_of(way):
        return (z, x, at_y(1 if way == 0 else -1), c)

    def pass_on(g, way, hop, j):
        if hop < hops(way, g):
            remote(
                ag.at[j, grp(g)],
                ag.at[j, grp(g)],
                send_sem.at[5],
                agr_sem.at[way, hop, g],
                side_of(way),
            )

    def across(g, j, rel):
        at = ny if rel == half and g >= G // HS else rel
        remote(ag.at[j, grp(g)], ag.at[j, grp(g)], send_sem.at[6], agd_sem.at[at], partner)

    for g in range(G):
        if g == 0:
            take(ag.at[me_j, pl.ds(1, per - 1)], disp_sem.at[0])
        else:
            take(ag.at[me_j, grp(g)], disp_sem.at[g])
        for way in range(2):
            pass_on(g, way, 0, me_j)
        across(g, me_j, 0)

    ready("wg")
    ready("wu")
    ready("gain")

    tall = slots // HS

    def absorb(rel, hs):
        yy = at_y(rel)
        other = 2 * yy + 1 - c
        part = pl.ds(hs * (ns // HS), ns // HS)
        if rel == half:
            take(ag.at[other, part], agd_sem.at[rel if hs == 0 else ny])
        elif hs == 0:
            take(ag.at[other], agd_sem.at[rel])
        cols = pl.ds(pl.multiple_of(yy * 2 * L, 2 * L), 2 * L)
        gain = gain_ref[:, cols]
        at = pl.ds(hs * tall, tall)
        lo = ag[2 * yy, part].reshape(tall, L).astype(F32)
        hi = ag[2 * yy + 1, part].reshape(tall, L).astype(F32)
        lhs = jnp.concatenate(
            [(lo * gain[:, :L]).astype(BF), (hi * gain[:, L:]).astype(BF)], axis=1
        )
        square = lo * lo + hi * hi
        if rel == 0:
            ssq[at, :] = square
            acc_g[at, :] = dot(lhs, wg[cols, :])
            acc_u[at, :] = dot(lhs, wu[cols, :])
        else:
            ssq[at, :] += square
            acc_g[at, :] += dot(lhs, wg[cols, :])
            acc_u[at, :] += dot(lhs, wu[cols, :])

    def catch(g, way, hop):
        rel = ny - hop - 1 if way == 0 else hop + 1
        j = 2 * at_y(rel) + c
        take(ag.at[j, grp(g)], agr_sem.at[way, hop, g])
        pass_on(g, way, hop + 1, j)
        across(g, j, rel)

    todo = [(0, hs) for hs in range(HS)]
    for hop in range(half - 1):
        for g in range(G):
            catch(g, 0, hop)
            catch(g, 1, hop)
            if g % 2 == 1 and todo:
                absorb(*todo.pop(0))
        while todo:
            absorb(*todo.pop(0))
        todo = [(rel, hs) for rel in (ny - hop - 1, hop + 1) for hs in range(HS)]

    def activate(hs):
        at = pl.ds(hs * tall, tall)
        scale = lax.rsqrt(jnp.sum(ssq[at, :], axis=1, keepdims=True) / (2 * ny * L) + 1e-06)
        gate = acc_g[at, :] * scale
        act_ref[at, :] = (gate / (1.0 + jnp.exp(-gate)) * (acc_u[at, :] * scale)).astype(BF)

    def project(hs):
        at = pl.ds(hs * tall, tall)
        act = act_ref[at, :]
        for rel in rels:
            o = dot(act, wd[rel])
            own2[rel, at, :] = o[:, :L]
            ps2[rel, at, :] = o[:, L:].astype(BF)
            remote(ps2.at[rel, at], pr2.at[rel, at], send_sem.at[7], p2_sem.at[rel, hs], partner)

    paired = set()

    def pair_ready(rel, hs):
        if (rel, hs) not in paired:
            paired.add((rel, hs))
            take(pr2.at[rel, pl.ds(hs * tall, tall)], p2_sem.at[rel, hs])

    def stage_of(stage, hs):
        for g in range(hs * (G // HS), (hs + 1) * (G // HS)):
            at = pl.ds(g * rows, rows)
            for way in range(2):
                begin = half - hops(way, g)
                if stage < begin:
                    continue
                rel = half - stage if way == 0 else (ny - half + stage) % ny
                pair_ready(rel, hs)
                s = own2[rel, at, :] + pr2[rel, at, :].astype(F32)
                if stage > begin:
                    take(r2r.at[way, stage - 1, g], r2_sem.at[way, stage - 1, g])
                    s = s + r2r[way, stage - 1, g].astype(F32)
                r2s[way, stage, g] = s.astype(BF)
                remote(
                    r2s.at[way, stage, g],
                    r2r.at[way, stage, g],
                    send_sem.at[8],
                    r2_sem.at[way, stage, g],
                    side_of(way),
                )

    for g in range(G // HS):
        catch(g, g % 2, half - 1)
        if todo:
            absorb(*todo.pop(0))
    while todo:
        absorb(*todo.pop(0))
    absorb(half, 0)
    activate(0)
    for g in range(G // HS, G):
        catch(g, g % 2, half - 1)
    pending.append((ag.at[pl.ds(0, ny - 1)], send_sem.at[5]))
    pending.append((ag.at[pl.ds(0, ny)], send_sem.at[6]))
    ready("wd")
    project(0)
    absorb(half, 1)
    activate(1)
    stage_of(0, 0)
    project(1)
    pending.append((ps2, send_sem.at[7]))
    stage_of(0, 1)
    for stage in range(1, half):
        for hs in range(HS):
            stage_of(stage, hs)
    for g in range(G):
        pair_ready(0, g // (G // HS))
        at = pl.ds(g * rows, rows)
        s = own2[0, at, :] + pr2[0, at, :].astype(F32)
        for way in range(2):
            take(r2r.at[way, half - 1, g], r2_sem.at[way, half - 1, g])
            s = s + r2r[way, half - 1, g].astype(F32)
        out2[grp(g)] = s.astype(BF).reshape(per, cap, L)
        for p in reversed(range(g * per, (g + 1) * per)):
            if p == 0:
                ret[me_s] = out2[0]
                continue
            tz, tx = sp_at(-pos[p][0], -pos[p][1])
            remote(out2.at[p], ret.at[me_s], send_sem.at[9], ret_sem.at[0], (tz, tx, y, c))
    pending.append((ps2.at[pl.ds(0, ny - 1)], send_sem.at[8]))
    pending.append((out2.at[pl.ds(0, ns - 1)], send_sem.at[9]))
    take(ret.at[pl.ds(0, ns - 1)], ret_sem.at[0])
    back = ret[...].reshape(slots, L)
    mix = rate_ref[0] * dot(p0_ref[...], back) + rate_ref[1] * dot(p1_ref[...], back)
    fin[me_j] = (state_ref[...].astype(F32) + mix).astype(BF)

    def write(j):
        pltpu.make_async_copy(fin.at[j], out_hbm.at[:, lane_block(j)], loc_sem.at[5]).start()

    for rel in rels[:-1]:
        remote(fin.at[me_j], fin.at[me_j], send_sem.at[10], fin_sem.at[rel], (z, x, at_y(rel), c))
    remote(fin.at[me_j], fin.at[me_j], send_sem.at[11], find_sem.at[0], partner)
    write(me_j)
    for rel in rels[-2::-1]:
        j = 2 * at_y(-rel) + c
        take(fin.at[j], fin_sem.at[rel])
        remote(fin.at[j], fin.at[j], send_sem.at[11], find_sem.at[rel], partner)
        write(j)
    for rel in rels[::-1]:
        j = 2 * at_y(-rel) + 1 - c
        take(fin.at[j], find_sem.at[rel])
        write(j)

    pending.append((fin.at[pl.ds(0, ny - 1)], send_sem.at[10]))
    pending.append((fin.at[pl.ds(0, ny)], send_sem.at[11]))
    pending.append((out_hbm, loc_sem.at[5]))
    for ref, sem in pending:
        take(ref, sem)

    @pl.when(me_s < ns - 1)
    def _():
        take(kv_ref, send_sem.at[0])


def per_device(
    dims,
    queries,
    key_rows,
    value_rows,
    sink_logits,
    out_weight,
    residual,
    norm_gain,
    routes,
    route_weights,
    gate_weight,
    up_weight,
    down_weight,
):
    nz, nx, ny = dims
    ns = nz * nx
    width = residual.shape[1]
    hidden = gate_weight.shape[2]
    cap = 2 * T * TOP // ns
    slots = ns * cap
    rows = slots // G
    half = ny // 2
    hbm = pl.BlockSpec(memory_space=pl.ANY)
    sm = pl.BlockSpec(memory_space=pltpu.SMEM)
    scratch = [
        pltpu.VMEM((T, L), BF),
        pltpu.VMEM((2, HEAD_DIM, T), BF),
        pltpu.VMEM((1, width), F32),
        pltpu.VMEM((TOP, T), jnp.int32),
        pltpu.VMEM((TOP, T), F32),
        pltpu.VMEM((TOP, T, L), F32),
        pltpu.VMEM((ny, T, 2 * L), BF),
        pltpu.VMEM((width, hidden), BF),
        pltpu.VMEM((width, hidden), BF),
        pltpu.VMEM((ny, hidden, 2 * L), BF),
        pltpu.VMEM((T, L), BF),
        pltpu.VMEM((2, HEAD_DIM, T), BF),
        pltpu.VMEM((2, HEAD_DIM, T), BF),
        pltpu.VMEM((T, slots), BF),
        pltpu.VMEM((T, slots), BF),
        pltpu.VMEM((slots, T), BF),
        pltpu.VMEM((ny, T, L), F32),
        pltpu.VMEM((ny, T, L), BF),
        pltpu.VMEM((ny, T, L), BF),
        pltpu.VMEM((ny, T, L), BF),
        pltpu.VMEM((ny, T, L), BF),
        pltpu.VMEM((T, L), BF),
        pltpu.VMEM((ns, cap, L), BF),
        pltpu.VMEM((2 * ny, ns, cap, L), BF),
        pltpu.VMEM((slots, hidden), F32),
        pltpu.VMEM((slots, hidden), F32),
        pltpu.VMEM((slots, L), F32),
        pltpu.VMEM((slots, hidden), BF),
        pltpu.VMEM((ny, slots, L), F32),
        pltpu.VMEM((ny, slots, L), BF),
        pltpu.VMEM((ny, slots, L), BF),
        pltpu.VMEM((2, half, G, rows, L), BF),
        pltpu.VMEM((2, half, G, rows, L), BF),
        pltpu.VMEM((ns, cap, L), BF),
        pltpu.VMEM((ns, cap, L), BF),
        pltpu.VMEM((2 * ny, T, L), BF),
        pltpu.SemaphoreType.DMA((12,)),
        pltpu.SemaphoreType.DMA((12,)),
        pltpu.SemaphoreType.DMA((1,)),
        pltpu.SemaphoreType.DMA((ny,)),
        pltpu.SemaphoreType.DMA((ny,)),
        pltpu.SemaphoreType.DMA((G,)),
        pltpu.SemaphoreType.DMA((2, half, G)),
        pltpu.SemaphoreType.DMA((ny + 1,)),
        pltpu.SemaphoreType.DMA((ny, HS)),
        pltpu.SemaphoreType.DMA((2, half, G)),
        pltpu.SemaphoreType.DMA((1,)),
        pltpu.SemaphoreType.DMA((ny,)),
        pltpu.SemaphoreType.DMA((ny,)),
        pltpu.SemaphoreType.REGULAR((max(1, (ns // 2).bit_length() - 1),)),
    ]
    return pl.pallas_call(
        functools.partial(layer, dims),
        out_shape=jax.ShapeDtypeStruct((T, width), BF),
        in_specs=[hbm, hbm, hbm, sm] + [hbm] * 8,
        out_specs=hbm,
        scratch_shapes=scratch,
        compiler_params=pltpu.CompilerParams(
            collective_id=0, has_side_effects=True, vmem_limit_bytes=67043328
        ),
        name="layer",
    )(
        queries,
        key_rows.T,
        value_rows.T,
        sink_logits,
        out_weight,
        residual,
        norm_gain.reshape(1, width),
        routes.T,
        route_weights.T,
        gate_weight,
        up_weight,
        down_weight,
    )


def build(devices, dims):
    torus = Mesh(devices.reshape(*dims, 2), ("z", "x", "y", "c"))
    sp, tp = ("z", "x"), ("y", "c")
    placed = (
        P(sp, tp),
        P(sp, tp),
        P(sp, tp),
        P(tp),
        P(tp, None),
        P(sp, None),
        P(),
        P(sp, None),
        P(sp, None),
        P(sp, None, tp),
        P(sp, None, tp),
        P(sp, tp, None),
    )
    return jax.shard_map(
        functools.partial(per_device, dims),
        mesh=torus,
        in_specs=placed,
        out_specs=P(sp, None),
        check_vma=False,
    )


def solution(mesh):
    sp, tp = mesh.shape["sp"], mesh.shape["tp"]
    return build(mesh.devices, (sp // NX, NX, tp // 2))
```

```python
import functools

import jax
import jax.numpy as jnp
from jax import lax
from jax.experimental import pallas as pl
from jax.experimental.pallas import tpu as pltpu
from jax.sharding import Mesh
from jax.sharding import PartitionSpec as P

HEAD_DIM = 64
QH = 32
TOP = 2
T = 128
L = 128
G = 8
HS = 2
BF = jnp.bfloat16
F32 = jnp.float32
NX = 4


def dot(a, b, dims=((1,), (0,))):
    return lax.dot_general(a, b, (dims, ((), ())), preferred_element_type=F32)


def offsets(nz, nx):
    def far(k):
        dz, dx = k // nx, k % nx
        return min(dz, nz - dz) + min(dx, nx - dx)

    return [(k // nx, k % nx) for k in sorted(range(nz * nx), key=lambda k: (far(k), k))]


def layer(
    dims,
    q_hbm,
    k_hbm,
    v_hbm,
    sink_ref,
    wo_hbm,
    res_hbm,
    gain_hbm,
    routes_hbm,
    rw_hbm,
    wg_hbm,
    wu_hbm,
    wd_hbm,
    out_hbm,
    q_ref,
    kv_ref,
    gain_ref,
    routes_ref,
    rw_ref,
    rate_ref,
    wo,
    wg,
    wu,
    wd,
    res,
    halo,
    old_ref,
    p0_ref,
    p1_ref,
    pick_ref,
    own1,
    ps1,
    pr1,
    r1s,
    r1r,
    state_ref,
    disp,
    ag,
    acc_g,
    acc_u,
    ssq,
    act_ref,
    own2,
    ps2,
    pr2,
    r2s,
    r2r,
    out2,
    ret,
    fin,
    loc_sem,
    send_sem,
    halo_sem,
    p1_sem,
    r1_sem,
    disp_sem,
    agr_sem,
    agd_sem,
    p2_sem,
    r2_sem,
    ret_sem,
    fin_sem,
    find_sem,
    know_sem,
):
    nz, nx, ny = dims
    ns = nz * nx
    slots = ns * disp.shape[1]
    cap = disp.shape[1]
    half = ny // 2
    per = ns // G
    rows = slots // G
    z, x, y, c = (lax.axis_index(a) for a in ("z", "x", "y", "c"))
    me_s = z * nx + x
    me_j = 2 * y + c
    pos = offsets(nz, nx)

    def at_y(rel):
        return lax.rem(y + (rel + ny) % ny, ny)

    def sp_at(dz, dx):
        return lax.rem(z + dz % nz, nz), lax.rem(x + dx % nx, nx)

    partner = (z, x, y, 1 - c)

    def remote(src, dst, s, r, dev):
        cp = pltpu.make_async_remote_copy(
            src_ref=src,
            dst_ref=dst,
            send_sem=s,
            recv_sem=r,
            device_id=dev,
            device_id_type=pl.DeviceIdType.MESH,
        )
        cp.start()

    def take(ref, sem):
        pltpu.make_async_copy(ref, ref, sem).wait()

    barrier = pltpu.get_barrier_semaphore()

    def along(d):
        at = lax.rem(me_s + d + ns, ns)
        return at // nx, lax.rem(at, nx), y, c

    def signal(sem, dev):
        pl.semaphore_signal(sem, inc=1, device_id=dev, device_id_type=pl.DeviceIdType.MESH)

    signal(barrier, along(1))
    signal(barrier, along(-1))
    signal(barrier, partner)
    for d in range(1, nz):
        signal(barrier, (*sp_at(d, 0), y, c))
    for d in range(1, nx):
        signal(barrier, (*sp_at(0, d), y, c))
    for rel in range(1, ny):
        signal(barrier, (z, x, at_y(rel), c))

    def lane_block(j):
        return pl.ds(pl.multiple_of(j * L, L), L)

    loads = {}

    def load(name, src, dst, sem):
        pltpu.make_async_copy(src, dst, loc_sem.at[sem]).start()
        loads[name] = (dst, loc_sem.at[sem])

    def ready(name):
        take(*loads.pop(name))

    pending = []

    load("k", k_hbm, kv_ref.at[0], 6)
    load("v", v_hbm, kv_ref.at[1], 7)
    load("q", q_hbm, q_ref, 8)
    load("routes", routes_hbm, routes_ref, 9)
    load("rw", rw_hbm, rw_ref, 10)
    load("gain", gain_hbm, gain_ref, 11)
    load("res", res_hbm.at[:, lane_block(me_j)], res, 0)
    for rel in range(ny):
        for side in range(2):
            j = 2 * at_y(rel) + (c if side == 0 else 1 - c)
            pltpu.make_async_copy(
                wo_hbm.at[:, lane_block(j)], wo.at[rel, :, pl.ds(side * L, L)], loc_sem.at[1]
            ).start()
    loads["wo"] = (wo, loc_sem.at[1])
    load("wg", wg_hbm.at[0], wg, 2)
    load("wu", wu_hbm.at[0], wu, 3)
    for rel in range(ny):
        for side in range(2):
            j = 2 * at_y(rel) + (c if side == 0 else 1 - c)
            pltpu.make_async_copy(
                wd_hbm.at[0, :, lane_block(j)], wd.at[rel, :, pl.ds(side * L, L)], loc_sem.at[4]
            ).start()
    loads["wd"] = (wd, loc_sem.at[4])

    ready("routes")
    ready("rw")
    lanes = lax.broadcasted_iota(jnp.int32, (T, L), 1)
    subs = lax.broadcasted_iota(jnp.int32, (T, L), 0)
    experts = lax.broadcasted_iota(jnp.int32, (ns, T), 0)
    slot_ids = lax.broadcasted_iota(jnp.int32, (slots, T), 0).astype(F32)
    earlier = jnp.where(subs < lanes, 1.0, 0.0).astype(BF)
    chosen = [routes_ref[t : t + 1, :] for t in range(TOP)]
    named = [e == experts for e in chosen]
    member = jnp.where(named[0] | named[1], 1.0, 0.0).astype(BF)
    before = dot(member, earlier)
    picks = []
    for t in range(TOP):
        rank = jnp.sum(jnp.where(named[t], before, 0.0), axis=0, keepdims=True)
        picks.append(jnp.where(slot_ids == chosen[t].astype(F32) * cap + rank, 1.0, 0.0))
        rate_ref[t] = jnp.transpose(jnp.broadcast_to(rw_ref[t : t + 1, :], (L, T)))
    p0_ref[...] = jnp.transpose(picks[0]).astype(BF)
    p1_ref[...] = jnp.transpose(picks[1]).astype(BF)
    pick_ref[...] = (picks[0] + picks[1]).astype(BF)

    dist = (subs - lanes).astype(F32)
    ready("q")
    ready("k")
    ready("v")
    q = q_ref[...]
    head = 2 * me_j

    def masked(h, keys, gap, allowed):
        s = dot(q[:, h * HEAD_DIM : (h + 1) * HEAD_DIM], keys)
        idx = jnp.full((T, L), head + h + 1, jnp.int32).astype(F32)
        slope = jnp.exp2(-8.0 * idx / QH)
        return jnp.where(allowed, s * HEAD_DIM**-0.5 - slope * gap, -1e30)

    own_s = [masked(h, kv_ref[0], dist, lanes <= subs) for h in range(2)]

    pl.semaphore_wait(barrier, nz + nx + ny)
    for d in range(1, nz):
        signal(know_sem, (*sp_at(d, 0), y, c))

    @pl.when(me_s < ns - 1)
    def _():
        remote(kv_ref, halo, send_sem.at[0], halo_sem.at[0], along(1))

    @pl.when(me_s > 0)
    def _():
        take(halo, halo_sem.at[0])
        old_ref[...] = halo[...]

    @pl.when(me_s == 0)
    def _():
        old_ref[...] = kv_ref[...]

    v_own = kv_ref[1]
    k_old = old_ref[0]
    v_old = old_ref[1]
    parts = []
    for h in range(2):
        old_s = masked(h, k_old, dist + T, (lanes >= subs) & (me_s > 0))
        peak = jnp.maximum(
            jnp.max(own_s[h], axis=1, keepdims=True), jnp.max(old_s, axis=1, keepdims=True)
        )
        total = jnp.sum(jnp.exp(own_s[h] - peak), axis=1, keepdims=True) + jnp.sum(
            jnp.exp(old_s - peak), axis=1, keepdims=True
        )
        log_total = peak + jnp.log(total)
        mixed = dot(jnp.exp(own_s[h] - log_total).astype(BF), v_own, ((1,), (1,))) + dot(
            jnp.exp(old_s - log_total).astype(BF), v_old, ((1,), (1,))
        )
        keep = 1.0 / (1.0 + jnp.exp(sink_ref[h] - log_total))
        parts.append((mixed * keep).astype(BF))
    attended = jnp.concatenate(parts, axis=1)

    rels = [half]
    for d in range(half - 1, 0, -1):
        rels += [d, ny - d]
    rels += [0]
    ready("wo")
    for rel in rels:
        o = dot(attended, wo[rel])
        own1[rel] = o[:, :L]
        ps1[rel] = o[:, L:].astype(BF)
        remote(ps1.at[rel], pr1.at[rel], send_sem.at[2], p1_sem.at[rel], partner)
    pending.append((ps1, send_sem.at[2]))
    for rel in rels[:-1]:
        take(pr1.at[rel], p1_sem.at[rel])
        r1s[rel] = (own1[rel] + pr1[rel].astype(F32)).astype(BF)
        remote(r1s.at[rel], r1r.at[rel], send_sem.at[3], r1_sem.at[rel], (z, x, at_y(rel), c))
    pending.append((r1s.at[pl.ds(0, ny - 1)], send_sem.at[3]))
    take(pr1.at[0], p1_sem.at[0])
    ready("res")
    total = res[...].astype(F32) + own1[0] + pr1[0].astype(F32)
    for rel in rels[-2::-1]:
        take(r1r.at[rel], r1_sem.at[rel])
        total = total + r1r[rel].astype(F32)
    state = total.astype(BF)
    state_ref[...] = state

    pl.semaphore_wait(know_sem, nz - 1)
    disp[...] = dot(pick_ref[...], state).astype(BF).reshape(ns, cap, L)
    for p in range(1, ns):
        tz, tx = sp_at(*pos[p])
        remote(
            disp.at[tz * nx + tx],
            ag.at[me_j, p],
            send_sem.at[4],
            disp_sem.at[p // per],
            (tz, tx, y, c),
        )
    ag[me_j, 0] = disp[me_s]
    pending.append((disp.at[pl.ds(0, ns - 1)], send_sem.at[4]))

    def grp(g):
        return pl.ds(g * per, per)

    def hops(way, g):
        return half if (way == 0) == (g % 2 == 0) else half - 1

    def side_of(way, d=1):
        return (z, x, at_y(d if way == 0 else -d), c)

    def far_group(g):
        return g >= G // HS

    def forward(g, way, dist, j, by):
        if dist <= hops(way, g):
            remote(
                ag.at[j, grp(g)],
                ag.at[j, grp(g)],
                send_sem.at[5],
                agr_sem.at[way, dist - 1, g],
                side_of(way, by),
            )

    def across(g, j, rel):
        remote(
            ag.at[j, grp(g)],
            ag.at[j, grp(g)],
            send_sem.at[6],
            agd_sem.at[rel, g // (G // HS)],
            partner,
        )

    for g in range(G):
        if g == 0:
            take(ag.at[me_j, pl.ds(1, per - 1)], disp_sem.at[0])
        else:
            take(ag.at[me_j, grp(g)], disp_sem.at[g])
        for way in range(2):
            if far_group(g):
                forward(g, way, 2, me_j, 2)
            forward(g, way, 1, me_j, 1)
        across(g, me_j, 0)

    ready("wg")
    ready("wu")
    ready("gain")

    tall = slots // HS

    def absorb(rel, hs):
        yy = at_y(rel)
        other = 2 * yy + 1 - c
        part = pl.ds(hs * (ns // HS), ns // HS)
        take(ag.at[other, part], agd_sem.at[rel, hs])
        cols = pl.ds(pl.multiple_of(yy * 2 * L, 2 * L), 2 * L)
        gain = gain_ref[:, cols]
        at = pl.ds(hs * tall, tall)
        lo = ag[2 * yy, part].reshape(tall, L).astype(F32)
        hi = ag[2 * yy + 1, part].reshape(tall, L).astype(F32)
        lhs = jnp.concatenate(
            [(lo * gain[:, :L]).astype(BF), (hi * gain[:, L:]).astype(BF)], axis=1
        )
        square = lo * lo + hi * hi
        if rel == 0:
            ssq[at, :] = square
            acc_g[at, :] = dot(lhs, wg[cols, :])
            acc_u[at, :] = dot(lhs, wu[cols, :])
        else:
            ssq[at, :] += square
            acc_g[at, :] += dot(lhs, wg[cols, :])
            acc_u[at, :] += dot(lhs, wu[cols, :])

    def catch(g, way, dist):
        rel = ny - dist if way == 0 else dist
        j = 2 * at_y(rel) + c
        take(ag.at[j, grp(g)], agr_sem.at[way, dist - 1, g])
        if not far_group(g):
            forward(g, way, dist + 1, j, 1)
        elif dist == 2:
            forward(g, way, 4, j, 2)
            forward(g, way, 3, j, 1)
        across(g, j, rel)

    def catch_all(hs, dist):
        for g in range(hs * (G // HS), (hs + 1) * (G // HS)):
            for way in range(2):
                if dist <= hops(way, g):
                    catch(g, way, dist)

    catch_all(0, 1)
    catch_all(0, 2)
    catch_all(1, 2)
    catch_all(1, 1)
    for rel in (0, 1, ny - 1):
        for hs in range(HS):
            absorb(rel, hs)
    catch_all(0, 3)
    for rel in (2, ny - 2):
        for hs in range(HS):
            absorb(rel, hs)
    catch_all(1, 3)

    def activate(hs):
        at = pl.ds(hs * tall, tall)
        scale = lax.rsqrt(jnp.sum(ssq[at, :], axis=1, keepdims=True) / (2 * ny * L) + 1e-06)
        gate = acc_g[at, :] * scale
        act_ref[at, :] = (gate / (1.0 + jnp.exp(-gate)) * (acc_u[at, :] * scale)).astype(BF)

    def project(hs):
        at = pl.ds(hs * tall, tall)
        act = act_ref[at, :]
        for rel in rels:
            o = dot(act, wd[rel])
            own2[rel, at, :] = o[:, :L]
            ps2[rel, at, :] = o[:, L:].astype(BF)
            remote(ps2.at[rel, at], pr2.at[rel, at], send_sem.at[7], p2_sem.at[rel, hs], partner)

    paired = set()

    def pair_ready(rel, hs):
        if (rel, hs) not in paired:
            paired.add((rel, hs))
            take(pr2.at[rel, pl.ds(hs * tall, tall)], p2_sem.at[rel, hs])

    def at_of(g):
        return pl.ds(g * rows, rows)

    def share(way, dist, g):
        rel = dist if way == 0 else (ny - dist) % ny
        pair_ready(rel, g // (G // HS))
        return own2[rel, at_of(g), :] + pr2[rel, at_of(g), :].astype(F32)

    def arrived(way, at, g):
        take(r2r.at[way, at, g], r2_sem.at[way, at, g])
        return r2r[way, at, g].astype(F32)

    def send_sum(s, way, at, g, by):
        r2s[way, at, g] = s.astype(BF)
        remote(
            r2s.at[way, at, g],
            r2r.at[way, at, g],
            send_sem.at[8],
            r2_sem.at[way, at, g],
            side_of(way, by),
        )

    def near_stage(stage):
        for g in range(G // HS):
            for way in range(2):
                begin = half - hops(way, g)
                if stage >= begin:
                    s = share(way, half - stage, g)
                    if stage > begin:
                        s = s + arrived(way, stage - 1, g)
                    send_sum(s, way, stage, g, 1)

    def far_start():
        for g in range(G // HS, G):
            for way in range(2):
                if hops(way, g) >= 4:
                    send_sum(share(way, 4, g), way, 1, g, 2)
                send_sum(share(way, 3, g), way, 0, g, 1)
        for g in range(G // HS, G):
            for way in range(2):
                send_sum(share(way, 1, g), way, 2, g, 1)

    def far_middle():
        for g in range(G // HS, G):
            for way in range(2):
                s = share(way, 2, g) + arrived(way, 0, g)
                if hops(way, g) >= 4:
                    s = s + arrived(way, 1, g)
                send_sum(s, way, 3, g, 2)

    def finish(g):
        s = share(0, 0, g)
        for way in range(2):
            if far_group(g):
                s = s + arrived(way, 2, g)
            s = s + arrived(way, 3, g)
        out2[grp(g)] = s.astype(BF).reshape(per, cap, L)
        for p in reversed(range(g * per, (g + 1) * per)):
            if p == 0:
                ret[me_s] = out2[0]
                continue
            tz, tx = sp_at(-pos[p][0], -pos[p][1])
            remote(out2.at[p], ret.at[me_s], send_sem.at[9], ret_sem.at[0], (tz, tx, y, c))

    for rel in (3, ny - 3):
        absorb(rel, 0)
    catch_all(0, 4)
    for rel in (3, ny - 3):
        absorb(rel, 1)
    absorb(half, 0)
    activate(0)
    catch_all(1, 4)
    pending.append((ag.at[pl.ds(0, ny - 1)], send_sem.at[5]))
    pending.append((ag.at[pl.ds(0, ny)], send_sem.at[6]))
    ready("wd")
    project(0)
    absorb(half, 1)
    activate(1)
    near_stage(0)
    project(1)
    pending.append((ps2, send_sem.at[7]))
    far_start()
    near_stage(1)
    far_middle()
    near_stage(2)
    near_stage(3)
    for g in reversed(range(G)):
        finish(g)
    pending.append((ps2.at[pl.ds(0, ny - 1)], send_sem.at[8]))
    pending.append((out2.at[pl.ds(0, ns - 1)], send_sem.at[9]))
    take(ret.at[pl.ds(0, ns - 1)], ret_sem.at[0])
    back = ret[...].reshape(slots, L)
    mix = rate_ref[0] * dot(p0_ref[...], back) + rate_ref[1] * dot(p1_ref[...], back)
    fin[me_j] = (state_ref[...].astype(F32) + mix).astype(BF)

    def write(j):
        pltpu.make_async_copy(fin.at[j], out_hbm.at[:, lane_block(j)], loc_sem.at[5]).start()

    for rel in rels[:-1]:
        remote(fin.at[me_j], fin.at[me_j], send_sem.at[10], fin_sem.at[rel], (z, x, at_y(rel), c))
    remote(fin.at[me_j], fin.at[me_j], send_sem.at[11], find_sem.at[0], partner)
    write(me_j)
    for rel in rels[-2::-1]:
        j = 2 * at_y(-rel) + c
        take(fin.at[j], fin_sem.at[rel])
        remote(fin.at[j], fin.at[j], send_sem.at[11], find_sem.at[rel], partner)
        write(j)
    for rel in rels[::-1]:
        j = 2 * at_y(-rel) + 1 - c
        take(fin.at[j], find_sem.at[rel])
        write(j)

    pending.append((fin.at[pl.ds(0, ny - 1)], send_sem.at[10]))
    pending.append((fin.at[pl.ds(0, ny)], send_sem.at[11]))
    pending.append((out_hbm, loc_sem.at[5]))
    for ref, sem in pending:
        take(ref, sem)

    @pl.when(me_s < ns - 1)
    def _():
        take(kv_ref, send_sem.at[0])


def per_device(
    dims,
    queries,
    key_rows,
    value_rows,
    sink_logits,
    out_weight,
    residual,
    norm_gain,
    routes,
    route_weights,
    gate_weight,
    up_weight,
    down_weight,
):
    nz, nx, ny = dims
    ns = nz * nx
    width = residual.shape[1]
    hidden = gate_weight.shape[2]
    cap = 2 * T * TOP // ns
    slots = ns * cap
    rows = slots // G
    half = ny // 2
    hbm = pl.BlockSpec(memory_space=pl.ANY)
    sm = pl.BlockSpec(memory_space=pltpu.SMEM)
    scratch = [
        pltpu.VMEM((T, L), BF),
        pltpu.VMEM((2, HEAD_DIM, T), BF),
        pltpu.VMEM((1, width), F32),
        pltpu.VMEM((TOP, T), jnp.int32),
        pltpu.VMEM((TOP, T), F32),
        pltpu.VMEM((TOP, T, L), F32),
        pltpu.VMEM((ny, T, 2 * L), BF),
        pltpu.VMEM((width, hidden), BF),
        pltpu.VMEM((width, hidden), BF),
        pltpu.VMEM((ny, hidden, 2 * L), BF),
        pltpu.VMEM((T, L), BF),
        pltpu.VMEM((2, HEAD_DIM, T), BF),
        pltpu.VMEM((2, HEAD_DIM, T), BF),
        pltpu.VMEM((T, slots), BF),
        pltpu.VMEM((T, slots), BF),
        pltpu.VMEM((slots, T), BF),
        pltpu.VMEM((ny, T, L), F32),
        pltpu.VMEM((ny, T, L), BF),
        pltpu.VMEM((ny, T, L), BF),
        pltpu.VMEM((ny, T, L), BF),
        pltpu.VMEM((ny, T, L), BF),
        pltpu.VMEM((T, L), BF),
        pltpu.VMEM((ns, cap, L), BF),
        pltpu.VMEM((2 * ny, ns, cap, L), BF),
        pltpu.VMEM((slots, hidden), F32),
        pltpu.VMEM((slots, hidden), F32),
        pltpu.VMEM((slots, L), F32),
        pltpu.VMEM((slots, hidden), BF),
        pltpu.VMEM((ny, slots, L), F32),
        pltpu.VMEM((ny, slots, L), BF),
        pltpu.VMEM((ny, slots, L), BF),
        pltpu.VMEM((2, half, G, rows, L), BF),
        pltpu.VMEM((2, half, G, rows, L), BF),
        pltpu.VMEM((ns, cap, L), BF),
        pltpu.VMEM((ns, cap, L), BF),
        pltpu.VMEM((2 * ny, T, L), BF),
        pltpu.SemaphoreType.DMA((12,)),
        pltpu.SemaphoreType.DMA((12,)),
        pltpu.SemaphoreType.DMA((1,)),
        pltpu.SemaphoreType.DMA((ny,)),
        pltpu.SemaphoreType.DMA((ny,)),
        pltpu.SemaphoreType.DMA((G,)),
        pltpu.SemaphoreType.DMA((2, half, G)),
        pltpu.SemaphoreType.DMA((ny, HS)),
        pltpu.SemaphoreType.DMA((ny, HS)),
        pltpu.SemaphoreType.DMA((2, half, G)),
        pltpu.SemaphoreType.DMA((1,)),
        pltpu.SemaphoreType.DMA((ny,)),
        pltpu.SemaphoreType.DMA((ny,)),
        pltpu.SemaphoreType.REGULAR,
    ]
    return pl.pallas_call(
        functools.partial(layer, dims),
        out_shape=jax.ShapeDtypeStruct((T, width), BF),
        in_specs=[hbm, hbm, hbm, sm] + [hbm] * 8,
        out_specs=hbm,
        scratch_shapes=scratch,
        compiler_params=pltpu.CompilerParams(
            collective_id=0, has_side_effects=True, vmem_limit_bytes=67043328
        ),
        name="layer",
    )(
        queries,
        key_rows.T,
        value_rows.T,
        sink_logits,
        out_weight,
        residual,
        norm_gain.reshape(1, width),
        routes.T,
        route_weights.T,
        gate_weight,
        up_weight,
        down_weight,
    )


def build(devices, dims):
    torus = Mesh(devices.reshape(*dims, 2), ("z", "x", "y", "c"))
    sp, tp = ("z", "x"), ("y", "c")
    placed = (
        P(sp, tp),
        P(sp, tp),
        P(sp, tp),
        P(tp),
        P(tp, None),
        P(sp, None),
        P(),
        P(sp, None),
        P(sp, None),
        P(sp, None, tp),
        P(sp, None, tp),
        P(sp, tp, None),
    )
    return jax.shard_map(
        functools.partial(per_device, dims),
        mesh=torus,
        in_specs=placed,
        out_specs=P(sp, None),
        check_vma=False,
    )


def solution(mesh):
    sp, tp = mesh.shape["sp"], mesh.shape["tp"]
    return build(mesh.devices, (sp // NX, NX, tp // 2))
```
